32 devices in a mesh: ep: 8 (over z, x), tp: 4 (over y, core).
Axes of the slice: x: 2, y: 2, z: 4, core: 2. Of those that a mesh axis runs over, the one named last changes fastest.
Arguments:
- mixer_group_input: bfloat16 [2048, 1024], P('ep', 'tp'), may hold values from -6 to 6
- log_step_size: float32 [64, 2048], P('tp', 'ep'), may hold values from -16 to 0
- extra_log_decay: float32 [64, 2048], P('tp', 'ep'), may hold values from -0.7 to 0
- negated_eigen_real: float32 [64, 64], P('tp'), may hold values from 0.35 to 0.7
- frequency: float32 [64, 64], P('tp'), may hold values from 0 to 200
- group_input_matrices: bfloat16 [2, 64, 64, 16], P(None, 'tp'), may hold values from -1.5 to 1.5
- group_output_matrices: bfloat16 [2, 64, 16, 64], P(None, 'tp'), may hold values from -0.5 to 0.5
- channel_feedthrough: float32 [1024], P('tp'), may hold values from -3 to 3
- mixer_norm_scale: float32 [1024], replicated, may hold values from 0.1 to 1.9
- mixer_output_weight: bfloat16 [1024, 2048], P(None, 'tp'), may hold values from -0.1875 to 0.1875
- second_micro_input: bfloat16 [1024, 2048], P('ep'), may hold values from -6 to 6
- expert_norm_scale: float32 [2048], replicated, may hold values from 0.1 to 1.9
- routes: int32 [1024, 4], P('ep'), may hold values from 0 to 7, all different within a row; in each aligned block of 128 rows (0 to 127, 128 to 255, ...) at most 128 rows name the same one
- chosen_expert_weight: float32 [1024, 4], P('ep'), may hold values from 0.1 to 1
- expert_gate_weight: bfloat16 [8, 2048, 2048], P('ep', None, 'tp'), may hold values from -0.125 to 0.125
- expert_up_weight: bfloat16 [8, 2048, 2048], P('ep', None, 'tp'), may hold values from -0.125 to 0.125
- expert_down_weight: bfloat16 [8, 2048, 2048], P('ep', None, 'tp'), may hold values from -0.125 to 0.125
- shared_gate_weight: bfloat16 [2048, 2048], P(None, 'tp'), may hold values from -0.125 to 0.125
- shared_up_weight: bfloat16 [2048, 2048], P(None, 'tp'), may hold values from -0.125 to 0.125
- shared_down_weight: bfloat16 [2048, 2048], P(None, 'tp'), may hold values from -0.125 to 0.125
Outputs:
- mixed: bfloat16 [2048, 2048], P('ep', 'tp')
- moe_out: bfloat16 [1024, 2048], P('ep', 'tp')
The draws below stay inside these ranges and needn't reach their ends.
Inputs may be any that keep to these rules, and one draw needn't show every extreme that they name: `routes`: each row names 4 different experts; in each aligned block of 128 rows no expert is named by more than 128 rows, and in some block one expert is named by exactly 128 rows.
All inputs are finite; a program needn't handle non-finite values.
Results may differ from the reference program's by a relative error of at most 0.0068.
Values may be sent and summed in bfloat16 or wider, within the bound.
A program may use at most 192 MiB of HBM per device.

```python
import math
import jax
import jax.numpy as jnp
import numpy as np
from jax import lax

D = 2048
GROUPS = 64
GROUP_CH = 16
STATE = 64
WIDTH_SSM = 1024
FE = 2048
TOP_K = 4
TOKENS_PER_SHARD = 256
TOK_EP2 = 128
EXPERTS = 8
CAP = 128
TOKENS1 = 2048
TOKENS2 = 1024
N_EP = 8


def draw_log_step_size(key, part):
    base_key = jax.random.fold_in(key, 101)
    slow_key, fast_key, level_key, block_key, rough_key = jax.random.split(base_key, 5)
    slow_share = 0.5
    slow = jax.random.uniform(slow_key, (GROUPS,), jnp.float32) < slow_share
    fast_step = jax.random.uniform(fast_key, (GROUPS,), jnp.float32, 0.045, 0.09)
    slow_step = jax.random.uniform(level_key, (GROUPS,), jnp.float32, 0.15, 0.3) / (0.7 * TOKENS1)
    base = jnp.log(jnp.where(slow, slow_step, fast_step))
    block_count = TOKENS1 // TOKENS_PER_SHARD
    block_factor = jax.random.uniform(block_key, (GROUPS, block_count), jnp.float32, -0.7, 0.7)
    rough = jax.random.uniform(rough_key, (GROUPS, TOKENS1), jnp.float32, -0.4, 0.4)
    return base[:, None] + jnp.repeat(block_factor, TOKENS_PER_SHARD, axis=1) + rough


def draw_extra_log_decay(key, part):
    base_key = jax.random.fold_in(key, 202)
    place_key, size_key = jax.random.split(base_key)
    places = jax.random.randint(place_key, (GROUPS, 2), 0, TOKENS1)
    sizes_log = jnp.log(jax.random.uniform(size_key, (GROUPS, 2), jnp.float32, 0.5, 0.8))
    positions = jnp.arange(TOKENS1, dtype=jnp.int32)
    hits = positions[None, :, None] == places[:, None, :]
    return jnp.sum(jnp.where(hits, sizes_log[:, None, :], 0.0), axis=2)


def block_scale(key, extent, cuts, least, top_value):
    loudness = 1.0
    for dim, blocks in cuts:
        heights = jax.random.uniform(jax.random.fold_in(jax.random.fold_in(key, 6), dim), (blocks,), jnp.float32, least / len(cuts), top_value / len(cuts))
        loudness = loudness * jnp.repeat(jnp.exp(heights), extent[dim] // blocks).reshape((-1,) + (1,) * (len(extent) - 1 - dim))
    return loudness


def shared_out(rng, own, number, rows, count, top, limit, slope):
    ranking = jax.random.permutation(rng, count)
    heavy_load, usual = shares(count, rows * top, limit, slope, True), shares(count, rows * top, limit, slope, False)
    places = jnp.arange(count)

    def named(lengths, turn):
        used = int((lengths > 0).sum())
        fixed = max(1, used // 4)
        shifted = fixed + (places - fixed + turn * (used - fixed)) % max(1, count - fixed)
        return jnp.zeros((count,), jnp.int32).at[ranking[jnp.where(places < fixed, places, shifted)]].set(jnp.asarray(lengths, jnp.int32))

    lengths = jnp.where(number % 4 == 0, named(heavy_load, number // 4), named(usual, number - number // 4 - 1))
    mixed = jax.random.permutation(jax.random.fold_in(own, 3), count)
    donor, sink = mixed[0:count // 2 * 2:2], mixed[1:count // 2 * 2:2]
    room = jnp.minimum(lengths[donor] - 1, limit - lengths[sink]) // 2
    room = jnp.where((donor == ranking[0]) | (sink == ranking[0]) | (lengths[sink] == 0), 0, jnp.maximum(room, 0))
    shifted = jax.random.randint(jax.random.fold_in(own, 4), (count // 2,), 0, 1 << 20) % (room + 1)
    lengths = lengths.at[donor].add(-shifted).at[sink].add(shifted)
    members = jnp.searchsorted(jnp.cumsum(lengths), jnp.arange(rows * top), side="right").astype(jnp.int32)
    listing = members.reshape(top, rows).T
    listing = listing[jax.random.permutation(jax.random.fold_in(own, 1), rows)]
    turn = jax.random.randint(jax.random.fold_in(own, 2), (rows, 1), 0, top)
    return jnp.take_along_axis(listing, (jnp.arange(top)[None, :] + turn) % top, axis=1)


def shares(amount, total, reach, lean, full):
    weights = [(1 << 20) // math.isqrt(rank ** lean) + 1 for rank in range(1, amount + 1)]
    largest = reach if full else min(reach, max(-(-total // amount), total * weights[0] // sum(weights)))
    least = 1 if total - largest >= amount - 1 else 0
    counts, rest = [largest] + [least] * (amount - 1), total - largest - least * (amount - 1)
    while rest > 0:
        free = [i for i in range(1, amount) if counts[i] < largest] or [i for i in range(1, amount) if counts[i] < reach]
        mass, remaining = sum([weights[i] for i in free]), rest
        for i in free:
            more = min(reach - counts[i], max(1, remaining * weights[i] // mass), rest)
            counts[i] = counts[i] + more
            rest = rest - more
    return np.array(counts)


def normal_values(rng, extent, scale, most, cuts=(), held_as=jnp.bfloat16):
    drawn = jax.random.normal(rng, extent, jnp.float32) * scale
    if len(cuts) > 0:
        drawn = block_scale(rng, extent, cuts, -0.22, 0.18) * drawn
    return jnp.clip(drawn, min=-most, max=most).astype(held_as)


def setup_inputs(seed: int = 0) -> dict:
    key_of = jax.random.split(jax.random.key(seed), 21)
    mixer_group_input = normal_values(key_of[0], (TOKENS1, WIDTH_SSM), 1.0, 6.0, ((0, 8), (1, 4)))
    log_step_size = draw_log_step_size(jax.random.fold_in(key_of[20], 71), 0)
    extra_log_decay = draw_extra_log_decay(jax.random.fold_in(key_of[20], 71), 0)
    negated_eigen_real = jnp.clip(jnp.exp(math.log(0.7) - 0.6931472 * jax.random.uniform(key_of[3], (GROUPS, STATE), jnp.float32) ** block_scale(key_of[3], (GROUPS, STATE), ((0, 4),), -0.2, 0.2)), 0.35, 0.7)
    frequency = jnp.clip(200.0 * jax.random.uniform(key_of[4], (GROUPS, STATE), jnp.float32) ** block_scale(key_of[4], (GROUPS, STATE), ((0, 4),), -0.2, 0.2), 0.0, 200.0)
    group_input_matrices = normal_values(key_of[5], (2, GROUPS, STATE, GROUP_CH), GROUP_CH ** -0.5, 1.5, ((1, 4),))
    group_output_matrices = normal_values(key_of[6], (2, GROUPS, GROUP_CH, STATE), (2 * STATE) ** -0.5, 0.5, ((1, 4),))
    channel_feedthrough = normal_values(key_of[7], (WIDTH_SSM,), 0.5, 3.0, ((0, 4),), jnp.float32)
    mixer_norm_scale = jnp.clip(1.0 + 0.18 * jax.random.normal(key_of[8], (WIDTH_SSM,), jnp.float32), 0.1, 1.9)
    mixer_output_weight = normal_values(key_of[9], (WIDTH_SSM, D), WIDTH_SSM ** -0.5, 0.1875, ((1, 4),))
    second_micro_input = normal_values(key_of[10], (TOKENS2, D), 1.0, 6.0, ((0, 8),))
    expert_norm_scale = jnp.clip(1.0 + 0.18 * jax.random.normal(key_of[11], (D,), jnp.float32), 0.1, 1.9)
    routes_keys = jax.random.split(jax.random.fold_in(key_of[12], 1), TOKENS2 // TOK_EP2)
    routes_turns = jax.random.permutation(jax.random.fold_in(key_of[12], 3), TOKENS2 // TOK_EP2)
    routes = jax.vmap(lambda own, number: shared_out(jax.random.fold_in(key_of[12], 2), own, number, TOK_EP2, EXPERTS, TOP_K, CAP, 1))(routes_keys, routes_turns).reshape((TOKENS2, TOP_K))
    chosen_expert_weight = jnp.clip(jnp.exp(math.log(1.0) - 2.3025851 * jax.random.uniform(key_of[13], (TOKENS2, TOP_K), jnp.float32) ** block_scale(key_of[13], (TOKENS2, TOP_K), ((0, 8),), -0.2, 0.2)), 0.1, 1.0)
    expert_gate_weight = normal_values(key_of[14], (EXPERTS, D, FE), D ** -0.5, 0.125, ((0, 8), (2, 4)))
    expert_up_weight = normal_values(key_of[15], (EXPERTS, D, FE), D ** -0.5, 0.125, ((0, 8), (2, 4)))
    expert_down_weight = normal_values(key_of[16], (EXPERTS, FE, D), FE ** -0.5, 0.125, ((0, 8), (2, 4)))
    shared_gate_weight = normal_values(key_of[17], (D, FE), D ** -0.5, 0.125, ((1, 4),))
    shared_up_weight = normal_values(key_of[18], (D, FE), D ** -0.5, 0.125, ((1, 4),))
    shared_down_weight = normal_values(key_of[19], (FE, D), FE ** -0.5, 0.125, ((1, 4),))
    return {"mixer_group_input": mixer_group_input, "log_step_size": log_step_size, "extra_log_decay": extra_log_decay, "negated_eigen_real": negated_eigen_real, "frequency": frequency, "group_input_matrices": group_input_matrices, "group_output_matrices": group_output_matrices, "channel_feedthrough": channel_feedthrough, "mixer_norm_scale": mixer_norm_scale, "mixer_output_weight": mixer_output_weight, "second_micro_input": second_micro_input, "expert_norm_scale": expert_norm_scale, "routes": routes, "chosen_expert_weight": chosen_expert_weight, "expert_gate_weight": expert_gate_weight, "expert_up_weight": expert_up_weight, "expert_down_weight": expert_down_weight, "shared_gate_weight": shared_gate_weight, "shared_up_weight": shared_up_weight, "shared_down_weight": shared_down_weight}


eps_norm = 1e-06

def combine_steps(earlier, latter):
    return (earlier[0] * latter[0] - earlier[1] * latter[1], earlier[0] * latter[1] + earlier[1] * latter[0], latter[0] * earlier[2] - latter[1] * earlier[3] + latter[2], latter[0] * earlier[3] + latter[1] * earlier[2] + latter[3])

def local_states(inputs, step_logs, losses, negated_eigen_real, frequency, group_input_matrices):
    positions = inputs.shape[0]
    group_list = negated_eigen_real.shape[0]
    channels = inputs.reshape(positions, group_list, -1).astype(jnp.float32)
    step_size = jnp.exp(step_logs).T
    decay_log = -negated_eigen_real[None, :, :] * step_size[:, :, None]
    magnitude = jnp.exp(decay_log + losses.T[:, :, None])
    rotation = frequency[None, :, :] * step_size[:, :, None]
    scaling = jnp.sqrt(-jnp.expm1(2.0 * decay_log))
    driven = jnp.einsum('tgc,rgpc->rtgp', channels, group_input_matrices.astype(jnp.float32), precision=lax.Precision.HIGHEST)
    return lax.associative_scan(combine_steps, (magnitude * jnp.cos(rotation), magnitude * jnp.sin(rotation), scaling * driven[0], scaling * driven[1]), axis=0)

def readout(state_real_part, state_imaginary, group_output_matrices, inputs, channel_feedthrough):
    positions = state_real_part.shape[0]
    mapped_result = jnp.einsum('fnx,njx->fnj', state_real_part, group_output_matrices[0].astype(jnp.float32), precision=lax.Precision.HIGHEST)
    mapped_result = mapped_result - jnp.einsum('fnx,njx->fnj', state_imaginary, group_output_matrices[1].astype(jnp.float32), precision=lax.Precision.HIGHEST)
    total = mapped_result.reshape(positions, -1) + channel_feedthrough * inputs.astype(jnp.float32)
    return jax.nn.gelu(total).astype(jnp.bfloat16)

def scaled_rows(values, gain):
    widened = values.astype(jnp.float32)
    factor = lax.rsqrt(lax.optimization_barrier(jnp.mean(widened * widened, axis=-1, keepdims=True)) + eps_norm)
    return (widened * factor * gain).astype(jnp.bfloat16)

def slot_table(block_routes, experts, capacity):
    flat_routes = block_routes.reshape(-1)
    onehot = (flat_routes[:, None] == jnp.arange(experts, dtype=jnp.int32)[None, :]).astype(jnp.int32)
    earlier_count = lax.optimization_barrier(jnp.sum((jnp.cumsum(onehot, axis=0) - onehot) * onehot, axis=1))
    return (flat_routes * capacity + earlier_count).astype(jnp.int32)

def fill_slots(token_rows, slot_index, slot_count, top_count):
    owner_row = jnp.zeros((slot_count,), jnp.int32).at[slot_index].set(jnp.arange(slot_index.shape[0], dtype=jnp.int32) // top_count)
    occupied = jnp.zeros((slot_count,), jnp.int32).at[slot_index].set(1)
    return jnp.where(occupied[:, None] > 0, token_rows[owner_row], jnp.zeros((), token_rows.dtype))

def expert_block(token_rows, gate_weight, up_weight, down_weight):
    gate_part = jnp.dot(token_rows, gate_weight, preferred_element_type=jnp.float32)
    up_part = jnp.dot(token_rows, up_weight, preferred_element_type=jnp.float32)
    hidden = (jax.nn.silu(gate_part) * up_part).astype(jnp.bfloat16)
    return jnp.dot(hidden, down_weight, preferred_element_type=jnp.float32)

def reference(mixer_group_input, log_step_size, extra_log_decay, negated_eigen_real, frequency, group_input_matrices, group_output_matrices, channel_feedthrough, mixer_norm_scale, mixer_output_weight, second_micro_input, expert_norm_scale, routes, chosen_expert_weight, expert_gate_weight, expert_up_weight, expert_down_weight, shared_gate_weight, shared_up_weight, shared_down_weight):
    channel_count = mixer_group_input.shape[1]
    group_list, states = negated_eigen_real.shape
    block_inputs = mixer_group_input.reshape(N_EP, TOKENS_PER_SHARD, channel_count)
    block_steps = log_step_size.reshape(group_list, N_EP, TOKENS_PER_SHARD).transpose(1, 0, 2)
    block_decay_terms = extra_log_decay.reshape(group_list, N_EP, TOKENS_PER_SHARD).transpose(1, 0, 2)

    def one_block(incoming, pieces):
        inputs, step_logs, losses = pieces
        reach_real, reach_imag, state_real_part, state_imaginary = local_states(inputs, step_logs, losses, negated_eigen_real, frequency, group_input_matrices)
        state_real_part = state_real_part + reach_real * incoming[0] - reach_imag * incoming[1]
        state_imaginary = state_imaginary + reach_real * incoming[1] + reach_imag * incoming[0]
        outputs = readout(state_real_part, state_imaginary, group_output_matrices, inputs, channel_feedthrough)
        return ((state_real_part[-1], state_imaginary[-1]), outputs)
    empty_state = jnp.zeros((group_list, states), jnp.float32)
    _, outputs = lax.scan(one_block, (empty_state, empty_state), (block_inputs, block_steps, block_decay_terms))
    ssm_out = outputs.reshape(N_EP * TOKENS_PER_SHARD, channel_count)
    normed_mix = scaled_rows(ssm_out, mixer_norm_scale)
    mixed = jnp.dot(normed_mix, mixer_output_weight, preferred_element_type=jnp.float32).astype(jnp.bfloat16)
    normed_tokens = scaled_rows(second_micro_input, expert_norm_scale)
    block_rows = normed_tokens.reshape(N_EP, TOK_EP2, D)
    slot_index = jax.vmap(lambda routes_block: slot_table(routes_block, EXPERTS, CAP))(routes.reshape(N_EP, TOK_EP2, TOP_K))
    sent = jax.vmap(lambda rows_block, slots_block: fill_slots(rows_block, slots_block, EXPERTS * CAP, TOP_K))(block_rows, slot_index)
    sent = sent.reshape(N_EP, EXPERTS, CAP, D)

    def one_expert(expert):
        arrived = lax.dynamic_index_in_dim(sent, expert, axis=1, keepdims=False).reshape(N_EP * CAP, D)
        result = expert_block(arrived, expert_gate_weight[expert], expert_up_weight[expert], expert_down_weight[expert])
        return result.astype(jnp.bfloat16).reshape(N_EP, CAP, D)
    results = lax.map(one_expert, jnp.arange(EXPERTS, dtype=jnp.int32))
    returned = results.transpose(1, 0, 2, 3).reshape(N_EP, EXPERTS * CAP, D)
    picked = jax.vmap(lambda back_block, slots_block: back_block[slots_block])(returned, slot_index)
    picked = picked.reshape(N_EP * TOK_EP2, TOP_K, D).astype(jnp.float32)
    shared = expert_block(normed_tokens, shared_gate_weight, shared_up_weight, shared_down_weight)
    moe_out = (shared + lax.optimization_barrier(jnp.sum(picked * chosen_expert_weight[:, :, None], axis=1))).astype(jnp.bfloat16)
    return (mixed, moe_out)
```

```python
import functools

import jax
import jax.numpy as jnp
from jax import lax
from jax.experimental import pallas as pl
from jax.experimental.pallas import tpu as pltpu
from jax.sharding import PartitionSpec as P

eps_norm = 1e-06
LANES = 128
ROWS = 8
MESH = pl.DeviceIdType.MESH
bf16, f32 = jnp.bfloat16, jnp.float32
COLUMN_LAG = 1
DOWN_LAG = 2
TILES_PER_STEP = 2
VMEM_BYTES = 62 * 1024 * 1024


def cos_sin(angle):
    turns = jnp.floor(angle * 0.6366197723675814 + 0.5)
    rest = ((angle - turns * 1.5703125) - turns * 4.837512969970703125e-4) - turns * 7.549789954891882e-8
    square = rest * rest
    sine = rest + rest * square * (
        -1.6666654611e-1 + square * (8.3321608736e-3 + square * -1.9515295891e-4)
    )
    cosine = (
        1.0
        - 0.5 * square
        + square
        * square
        * (
            4.166664568298827e-2
            + square * (-1.388731625493765e-3 + square * 2.443315711809948e-5)
        )
    )
    quarter = turns.astype(jnp.int32)
    odd = (quarter & 1) == 1
    out_cos = jnp.where(odd, sine, cosine)
    out_sin = jnp.where(odd, cosine, sine)
    out_cos = jnp.where(((quarter + 1) & 2) == 2, -out_cos, out_cos)
    out_sin = jnp.where((quarter & 2) == 2, -out_sin, out_sin)
    return out_cos, out_sin


def one_minus_exp_neg(y):
    series = y * (
        1.0
        - y * (1.0 / 2)
        * (1.0 - y * (1.0 / 3) * (1.0 - y * (1.0 / 4) * (1.0 - y * (1.0 / 5) * (1.0 - y * (1.0 / 6)))))
    )
    return jnp.where(y < 0.3, series, 1.0 - jnp.exp(-y))


def dot(a, b, dims=((1,), (0,)), precision=None):
    return lax.dot_general(a, b, (dims, ((), ())), preferred_element_type=f32, precision=precision)


def iota(shape, axis):
    return lax.broadcasted_iota(jnp.int32, shape, axis)


def ones_where(condition, dtype=bf16):
    return jnp.where(condition, 1.0, 0.0).astype(dtype)


def scaled_rows(values, gain):
    widened = values.astype(f32)
    factor = lax.rsqrt(jnp.mean(widened * widened, axis=-1, keepdims=True) + eps_norm)
    return (widened * factor * gain).astype(bf16)


def body(
    n_ep, n_tp,
    u_hbm, logs_hbm, loss_hbm, eig_hbm, freq_hbm, gin_hbm, gout_hbm, feed_hbm, mscale_hbm, mweight_hbm,
    x_hbm, gain_hbm, routes_hbm, chosen_hbm, gate_hbm, up_hbm, down_hbm, sgate_hbm, sup_hbm, sdown_hbm,
    mixed_ref, moe_ref,
    u, logs, loss, eig, freq, gin, gout, feed, mscale, mweight,
    x, gain, routes, chosen, gate, up, down, sgate, sup, sdown,
    tok, hid, res, ret, ends, ssm,
    us, parts, eigrow, freqrow, win, wout, ar_ref, ai_ref, br_ref, bi_ref, pre, inc, total, shared_cols, shares,
    load_sem,
    tok_up, tok_dn, tok_x, tok_sib, tok_recv, tok_recv_sib,
    hid_send_y, hid_send_sib, hid_recv_y, hid_recv_sib,
    res_send, res_recv, ends_send, ends_recv,
    ssm_sem,
):
    e, t = lax.axis_index("ep"), lax.axis_index("tp")
    n_line, n_y = n_ep // 2, n_tp // 2
    a, b = e // 2, e % 2
    y, c = t // 2, t % 2
    steps = n_ep
    token_rows, width = x.shape
    half = width // 2
    hidden = gate.shape[1]
    columns = down.shape[1]
    positions, channels = u.shape
    groups, states = eig.shape
    group_ch = channels // groups
    lanes_all = groups * states
    tiles = lanes_all // LANES
    per_tile = LANES // states
    segment = positions // ROWS

    barrier = pltpu.get_barrier_semaphore()
    for i in range(n_ep):
        @pl.when(e != i)
        def _():
            pl.semaphore_signal(barrier, inc=1, device_id={"ep": i, "tp": t}, device_id_type=MESH)
    for i in range(n_tp):
        @pl.when(t != i)
        def _():
            pl.semaphore_signal(barrier, inc=1, device_id={"ep": e, "tp": i}, device_id_type=MESH)

    pairs = [
        (x_hbm, x), (gain_hbm, gain), (sgate_hbm, sgate), (sup_hbm, sup), (gate_hbm.at[0], gate), (up_hbm.at[0], up),
        (u_hbm, u), (logs_hbm, logs), (loss_hbm, loss), (eig_hbm, eig), (freq_hbm, freq), (gin_hbm, gin),
        (gout_hbm, gout), (feed_hbm, feed), (down_hbm.at[0], down), (sdown_hbm, sdown), (mscale_hbm, mscale),
        (mweight_hbm, mweight), (routes_hbm, routes), (chosen_hbm, chosen),
    ]
    loads = [pltpu.make_async_copy(src, dst, load_sem.at[k]) for k, (src, dst) in enumerate(pairs)]
    for load in loads:
        load.start()

    left, right = a, n_line - 1 - a
    short = jnp.minimum(left, right)
    sign_long = jnp.where(left <= right, 1, -1)

    def near(k):
        odd = k % 2
        alternating = jnp.where(odd == 1, sign_long, -sign_long) * ((k + 1) // 2)
        beyond = sign_long * (k - short)
        return a + jnp.where(k <= 2 * short, alternating, beyond)

    def place(s):
        last = s == steps - 1
        odd = s % 2 == 1
        k = jnp.where(last, n_line - 1, jnp.where(odd, (s + 1) // 2, s // 2 - 1))
        other = jnp.where(last, 1, jnp.where(odd, 0, 1))
        k = jnp.where(s == 0, 0, k)
        other = jnp.where(s == 0, 0, other)
        row = jnp.where(k == 0, a, near(k))
        return row, other

    def block_of(row, other):
        return row * 2 + jnp.where(other == 1, 1 - b, b)

    def token_copy(blk, half_index, send, recv, ep, tp):
        part = tok.at[blk, :, pl.ds(pl.multiple_of(half_index * half, half), half)]
        return pltpu.make_async_remote_copy(
            part, part, send, recv, device_id={"ep": ep, "tp": tp}, device_id_type=MESH
        )

    sib = y * 2 + 1 - c

    def up_copy(row):
        return token_copy(row * 2 + b, c, tok_up.at[row], tok_recv.at[row * 2 + b], jnp.minimum(e + 2, n_ep - 2 + b), t)

    def dn_copy(row):
        return token_copy(row * 2 + b, c, tok_dn.at[row], tok_recv.at[row * 2 + b], jnp.maximum(e - 2, b), t)

    def x_copy(row):
        return token_copy(row * 2 + b, c, tok_x.at[row], tok_recv.at[row * 2 + b], a * 2 + 1 - b, t)

    def sib_copy(blk):
        return token_copy(blk, c, tok_sib.at[blk], tok_recv_sib.at[blk], e, sib)

    def forward(row):
        @pl.when((row <= a) & (a + 1 < n_line))
        def _():
            up_copy(row).start()

        @pl.when((row >= a) & (a >= 1))
        def _():
            dn_copy(row).start()

        x_copy(row).start()

    def hid_y_copy(s, yy):
        part = hid.at[s, c, y]
        return pltpu.make_async_remote_copy(
            part, part, hid_send_y.at[s], hid_recv_y.at[s], device_id={"ep": e, "tp": yy * 2 + c}, device_id_type=MESH
        )

    def hid_sib_copy(s, yy):
        part = hid.at[s, c, yy]
        return pltpu.make_async_remote_copy(
            part, part, hid_send_sib.at[s], hid_recv_sib.at[s], device_id={"ep": e, "tp": sib}, device_id_type=MESH
        )

    def span(ref, send, recv):
        return pltpu.make_async_remote_copy(
            ref, ref, send, recv, device_id={"ep": e, "tp": sib}, device_id_type=MESH
        )

    def gated(rows, gate_w, up_w, s):
        block = min(256, hidden)
        for n in range(hidden // block):
            cols = pl.ds(n * block, block)
            gate_part = dot(rows, gate_w[:, cols])
            up_part = dot(rows, up_w[:, cols])
            hid[s, c, y, :, cols] = (gate_part / (1.0 + jnp.exp(-gate_part)) * up_part).astype(bf16)

    def send_hidden(s):
        for dy in range(1, n_y):
            hid_y_copy(s, lax.rem(y + dy, n_y)).start()
        hid_sib_copy(s, y).start()

    def relay_hidden(s):
        span(hid.at[s, c, pl.ds(0, n_y - 1)], hid_send_y.at[s], hid_recv_y.at[s]).wait_recv()
        for dy in range(1, n_y):
            hid_sib_copy(s, lax.rem(y + dy, n_y)).start()

    def down_product(s, weight):
        span(hid.at[s, 1 - c], hid_send_sib.at[s], hid_recv_sib.at[s]).wait_recv()
        value = None
        for cc in range(2):
            for yy in range(n_y):
                rows = (yy * 2 + cc) * hidden
                term = dot(hid[s, cc, yy], weight[rows : rows + hidden, :])
                value = term if value is None else value + term
        return value

    def res_copy(blk):
        return pltpu.make_async_remote_copy(
            res.at[blk], ret.at[e], res_send.at[blk], res_recv.at[e], device_id={"ep": blk, "tp": t}, device_id_type=MESH
        )

    loads[0].wait()
    loads[1].wait()
    tok[e] = scaled_rows(x[...], gain[...])
    pl.semaphore_wait(barrier, n_ep + n_tp - 2)
    forward(a)

    loads[2].wait()
    loads[3].wait()
    gated(tok[e], sgate, sup, steps)
    send_hidden(steps)
    loads[4].wait()
    loads[5].wait()
    gated(tok[e], gate, up, 0)
    send_hidden(0)

    for k in range(6, 14):
        loads[k].wait()
    shuffle = ones_where(iota((positions, positions), 1) == (iota((positions, positions), 0) % ROWS) * segment + iota((positions, positions), 0) // ROWS)
    us[...] = dot(shuffle, u[...]).astype(bf16)
    parts[...] = jnp.zeros(parts.shape, bf16)
    slot = parts.shape[1] // 3
    for q, table in enumerate((jnp.exp(logs[...]), loss[...])):
        rest = table
        for r in range(3):
            piece = rest.astype(bf16)
            rest = rest - piece.astype(f32)
            parts[q, r * slot : r * slot + groups, :] = dot(piece, shuffle, ((1,), (1,))).astype(bf16)
    spread = ones_where(iota((states, LANES), 1) % states == iota((states, LANES), 0), f32)
    for table, rows_ref in ((eig, eigrow), (freq, freqrow)):
        wide = dot(table[...], spread, precision=lax.Precision.HIGHEST)
        row = jnp.zeros((tiles, LANES), f32)
        for h in range(per_tile):
            pick = ones_where(iota((tiles, groups), 1) == iota((tiles, groups), 0) * per_tile + h, f32)
            picked = dot(pick, wide, precision=lax.Precision.HIGHEST)
            row = jnp.where(iota((tiles, LANES), 1) // states == h, picked, row)
        rows_ref[...] = row
    spread_all = ones_where(iota((states, lanes_all), 1) % states == iota((states, lanes_all), 0))
    own_group = iota((channels, lanes_all), 0) // group_ch == iota((channels, lanes_all), 1) // states
    for r in range(2):
        win[r] = jnp.where(own_group, dot(gin[r], spread_all), 0.0).astype(bf16)
        wout[r] = jnp.where(own_group, dot(gout[r], spread_all), 0.0).astype(bf16)

    def tile_work(i):
        lanes = pl.ds(pl.multiple_of(i * LANES, LANES), LANES)
        slot_rows = 3 * slot
        own = iota((slot_rows, LANES), 0) % slot == per_tile * i + iota((slot_rows, LANES), 1) // states
        select = ones_where(own)
        step_wide = dot(parts[0], select, ((0,), (0,)))
        loss_wide = dot(parts[1], select, ((0,), (0,)))
        loss_rate = eigrow[pl.ds(i, 1), :] * step_wide
        magnitude = jnp.exp(loss_wide - loss_rate)
        cosine, sine = cos_sin(freqrow[pl.ds(i, 1), :] * step_wide)
        scaling = jnp.sqrt(one_minus_exp_neg(2.0 * loss_rate))
        ar_ref[:, lanes] = magnitude * cosine
        ai_ref[:, lanes] = magnitude * sine
        br_ref[:, lanes] = scaling * dot(us[...], win[0, :, lanes])
        bi_ref[:, lanes] = scaling * dot(us[...], win[1, :, lanes])
        reach = jnp.ones((ROWS, LANES), f32), jnp.zeros((ROWS, LANES), f32)
        state = jnp.zeros((ROWS, LANES), f32), jnp.zeros((ROWS, LANES), f32)
        for j in range(segment):
            at = pl.ds(j * ROWS, ROWS)
            ar, ai, br, bi = ar_ref[at, lanes], ai_ref[at, lanes], br_ref[at, lanes], bi_ref[at, lanes]
            reach = ar * reach[0] - ai * reach[1], ar * reach[1] + ai * reach[0]
            state = ar * state[0] - ai * state[1] + br, ar * state[1] + ai * state[0] + bi
            ar_ref[at, lanes] = reach[0]
            ai_ref[at, lanes] = reach[1]
            br_ref[at, lanes] = state[0]
            bi_ref[at, lanes] = state[1]
        row = iota((ROWS, LANES), 0)
        er, ei = jnp.ones((1, LANES), f32), jnp.zeros((1, LANES), f32)
        sr, si = jnp.zeros((1, LANES), f32), jnp.zeros((1, LANES), f32)
        pre_r = pre_i = pre_sr = pre_si = jnp.zeros((ROWS, LANES), f32)
        for k in range(ROWS):
            here = row == k
            pre_r = jnp.where(here, er, pre_r)
            pre_i = jnp.where(here, ei, pre_i)
            pre_sr = jnp.where(here, sr, pre_sr)
            pre_si = jnp.where(here, si, pre_si)
            tr, ti = reach[0][k : k + 1], reach[1][k : k + 1]
            ur, ui = state[0][k : k + 1], state[1][k : k + 1]
            er, ei, sr, si = (
                tr * er - ti * ei,
                tr * ei + ti * er,
                tr * sr - ti * si + ur,
                tr * si + ti * sr + ui,
            )
        for q, value in enumerate((pre_r, pre_i, pre_sr, pre_si)):
            pre[q, i] = value
        for q, value in enumerate((er, ei, sr, si)):
            ends[e, q, pl.ds(i, 1), :] = value

    def ends_copy(i):
        return pltpu.make_async_remote_copy(
            ends.at[e], ends.at[e], ends_send.at[i], ends_recv.at[e], device_id={"ep": i, "tp": t}, device_id_type=MESH
        )

    def send_ends():
        for i in range(1, n_ep):
            @pl.when(i > e)
            def _():
                ends_copy(i).start()

    def incoming():
        zero = jnp.zeros((tiles, LANES), f32)
        inc[0] = zero
        inc[1] = zero
        for i in range(n_ep - 1):
            @pl.when(i < e)
            def _():
                part = ends.at[i]
                pltpu.make_async_remote_copy(
                    part, part, ends_send.at[i], ends_recv.at[i], device_id={"ep": e, "tp": sib}, device_id_type=MESH
                ).wait_recv()
                tr, ti, ur, ui = ends[i, 0], ends[i, 1], ends[i, 2], ends[i, 3]
                sr, si = inc[0], inc[1]
                inc[0] = tr * sr - ti * si + ur
                inc[1] = tr * si + ti * sr + ui

    def split(value):
        high = value.astype(bf16)
        return high, (value - high.astype(f32)).astype(bf16)

    def read_tile(i):
        lanes = pl.ds(pl.multiple_of(i * LANES, LANES), LANES)
        ir, ii = inc[0, pl.ds(i, 1), :], inc[1, pl.ds(i, 1), :]
        pre_r, pre_i, pre_sr, pre_si = pre[0, i], pre[1, i], pre[2, i], pre[3, i]
        enter_r = (pre_sr + pre_r * ir - pre_i * ii)[None]
        enter_i = (pre_si + pre_r * ii + pre_i * ir)[None]
        shape = (segment, ROWS, LANES)
        ar, ai = ar_ref[:, lanes].reshape(shape), ai_ref[:, lanes].reshape(shape)
        br, bi = br_ref[:, lanes].reshape(shape), bi_ref[:, lanes].reshape(shape)
        state_r = (br + ar * enter_r - ai * enter_i).reshape(positions, LANES)
        state_i = (bi + ar * enter_i + ai * enter_r).reshape(positions, LANES)
        wr, wi = wout[0, :, lanes], -wout[1, :, lanes]
        high_r, low_r = split(state_r)
        high_i, low_i = split(state_i)
        nt = ((1,), (1,))
        total[...] += (dot(high_r, wr, nt) + dot(low_r, wr, nt)) + (dot(high_i, wi, nt) + dot(low_i, wi, nt))

    def ssm_y_copy(yy):
        part = ssm.at[c, y]
        return pltpu.make_async_remote_copy(
            part, part, ssm_sem.at[0], ssm_sem.at[1], device_id={"ep": e, "tp": yy * 2 + c}, device_id_type=MESH
        )

    def ssm_sib_copy(yy):
        part = ssm.at[c, yy]
        return pltpu.make_async_remote_copy(
            part, part, ssm_sem.at[2], ssm_sem.at[3], device_id={"ep": e, "tp": sib}, device_id_type=MESH
        )

    def read_out():
        total[...] = feed[...] * us[...].astype(f32)
        lax.fori_loop(0, tiles, lambda i, _: (read_tile(i), 0)[1], 0)
        value = total[...]
        inner = 0.7978845608028654 * (value + 0.044715 * (value * value * value))
        result = (0.5 * value * (1.0 + jnp.tanh(inner))).astype(bf16)
        unshuffle = ones_where(iota((positions, positions), 1) == (iota((positions, positions), 0) % segment) * ROWS + iota((positions, positions), 0) // segment)
        ssm[c, y] = dot(unshuffle, result).astype(bf16)
        for dy in range(1, n_y):
            ssm_y_copy(lax.rem(y + dy, n_y)).start()
        ssm_sib_copy(y).start()

    for k in range(14, 20):
        loads[k].wait()

    mixer_steps = -(-tiles // TILES_PER_STEP)
    ends_step = mixer_steps + 1
    read_step = min(ends_step + 2, steps + DOWN_LAG - 1)

    def step_body(s, carry):
        @pl.when(s < steps)
        def _():
            row, other = place(s)
            blk = block_of(row, other)
            token_copy(blk, c, tok_sib.at[blk], tok_recv.at[blk], e, sib).wait_recv()

            @pl.when(other == 0)
            def _():
                forward(row)

            sib_copy(blk).start()

        for k in range(TILES_PER_STEP):
            i = (s - 1) * TILES_PER_STEP + k

            @pl.when(i < tiles)
            def _():
                tile_work(i)

        @pl.when(s == ends_step)
        def _():
            send_ends()

        @pl.when(s < steps)
        def _():
            row, other = place(s)
            blk = block_of(row, other)
            token_copy(blk, 1 - c, tok_sib.at[blk], tok_recv_sib.at[blk], e, sib).wait_recv()
            gated(tok[blk], gate, up, s)
            send_hidden(s)

        @pl.when(s == 1)
        def _():
            relay_hidden(steps)

        @pl.when(s - COLUMN_LAG < steps)
        def _():
            relay_hidden(s - COLUMN_LAG)

        @pl.when(s == read_step)
        def _():
            incoming()
            read_out()

        @pl.when(s >= DOWN_LAG)
        def _():
            row, other = place(s - DOWN_LAG)
            blk = block_of(row, other)
            value = down_product(s - DOWN_LAG, down).astype(bf16)

            @pl.when(blk == e)
            def _():
                ret[e] = value

            @pl.when(blk != e)
            def _():
                res[blk] = value
                res_copy(blk).start()

        return carry

    lax.fori_loop(1, steps + DOWN_LAG, step_body, 0)

    span(ssm.at[c, pl.ds(0, n_y - 1)], ssm_sem.at[0], ssm_sem.at[1]).wait_recv()
    for dy in range(1, n_y):
        ssm_sib_copy(lax.rem(y + dy, n_y)).start()
    shared_cols[...] = down_product(steps, sdown)
    span(ssm.at[1 - c], ssm_sem.at[2], ssm_sem.at[3]).wait_recv()
    squares = jnp.zeros((positions, 1), f32)
    for cc in range(2):
        for yy in range(n_y):
            piece = ssm[cc, yy].astype(f32)
            squares = squares + jnp.sum(piece * piece, axis=-1, keepdims=True)
    factor = lax.rsqrt(squares / (channels * n_tp) + eps_norm)

    def gain_of(tt):
        if channels % LANES == 0:
            return mscale[:, tt * channels : (tt + 1) * channels]
        return mscale[tt : tt + 1, :]

    value = None
    for cc in range(2):
        for yy in range(n_y):
            tt = yy * 2 + cc
            normed = (ssm[cc, yy].astype(f32) * factor * gain_of(tt)).astype(bf16)
            term = dot(normed, mweight[tt * channels : (tt + 1) * channels, :])
            value = term if value is None else value + term
    mixed_ref[...] = value.astype(bf16)

    taken = jnp.zeros((n_ep, token_rows), f32)
    for k in range(routes.shape[0]):
        taken = taken + jnp.where(iota((n_ep, token_rows), 0) == routes[k : k + 1, :], chosen[k : k + 1, :], 0.0)
    shares[...] = taken.T

    def combine(s, carry):
        row, other = place(s)
        i = block_of(row, other)

        @pl.when(i != e)
        def _():
            part = ret.at[i]
            pltpu.make_async_remote_copy(
                part, part, res_send.at[i], res_recv.at[i], device_id={"ep": e, "tp": sib}, device_id_type=MESH
            ).wait_recv()

        share = jnp.sum(jnp.where(iota((token_rows, n_ep), 1) == i, shares[...], 0.0), axis=1, keepdims=True)
        shared_cols[...] += ret[i].astype(f32) * share
        return carry

    lax.fori_loop(0, steps, combine, 0)
    moe_ref[...] = shared_cols[...].astype(bf16)

    def drain(s, carry):
        @pl.when(s != e)
        def _():
            token_copy(s, c, tok_sib.at[s], tok_recv_sib.at[s], e, sib).wait_send()
            res_copy(s).wait_send()

        @pl.when(s > e)
        def _():
            ends_copy(s).wait_send()

        return carry

    lax.fori_loop(0, n_ep, drain, 0)

    def drain_line(row, carry):
        @pl.when((row <= a) & (a + 1 < n_line))
        def _():
            up_copy(row).wait_send()

        @pl.when((row >= a) & (a >= 1))
        def _():
            dn_copy(row).wait_send()

        x_copy(row).wait_send()
        return carry

    lax.fori_loop(0, n_line, drain_line, 0)

    def drain_hidden(s, carry):
        span(hid.at[s, c, pl.ds(0, n_y - 1)], hid_send_y.at[s], hid_recv_y.at[s]).wait_send()
        span(hid.at[s, c], hid_send_sib.at[s], hid_recv_sib.at[s]).wait_send()
        return carry

    lax.fori_loop(0, steps + 1, drain_hidden, 0)
    span(ssm.at[c, pl.ds(0, n_y - 1)], ssm_sem.at[0], ssm_sem.at[1]).wait_send()
    span(ssm.at[c], ssm_sem.at[2], ssm_sem.at[3]).wait_send()


def on_device(*operands):
    (
        u, logs, losses, eigen, frequency, group_in, group_out, feed, mixer_scale, mixer_weight,
        x, gain, routes, chosen, gate, up, down, shared_gate, shared_up, shared_down,
    ) = operands
    n_ep, n_tp = lax.axis_size("ep"), lax.axis_size("tp")
    positions, channels = u.shape
    groups, states = eigen.shape
    lanes_all = groups * states
    tiles = lanes_all // LANES
    token_rows, width = x.shape
    hidden, columns = gate.shape[2], down.shape[2]
    group_in = group_in.transpose(0, 1, 3, 2).reshape(2, channels, states)
    group_out = group_out.reshape(2, channels, states)
    feed = feed.reshape(1, channels)
    mixer_scale = mixer_scale.reshape((1, -1) if channels % LANES == 0 else (n_tp, channels))
    gain = gain.reshape(1, width)
    routes, chosen = routes.T, chosen.T
    given = (
        u, logs, losses, eigen, frequency, group_in, group_out, feed, mixer_scale, mixer_weight,
        x, gain, routes, chosen, gate, up, down, shared_gate, shared_up, shared_down,
    )
    local = [
        pltpu.VMEM(g.shape[1:] if k in (14, 15, 16) else g.shape, g.dtype) for k, g in enumerate(given)
    ]
    slot = -(-groups // 16) * 16
    wide = pltpu.VMEM((positions, lanes_all), f32)
    dma = pltpu.SemaphoreType.DMA
    scratch = local + [
        pltpu.VMEM((n_ep, token_rows, width), bf16),
        pltpu.VMEM((n_ep + 1, 2, n_tp // 2, token_rows, hidden), bf16),
        pltpu.VMEM((n_ep, token_rows, columns), bf16),
        pltpu.VMEM((n_ep, token_rows, columns), bf16),
        pltpu.VMEM((n_ep, 4, tiles, LANES), f32),
        pltpu.VMEM((2, n_tp // 2, positions, channels), bf16),
        pltpu.VMEM((positions, channels), bf16),
        pltpu.VMEM((2, 3 * slot, positions), bf16),
        pltpu.VMEM((tiles, LANES), f32),
        pltpu.VMEM((tiles, LANES), f32),
        pltpu.VMEM((2, channels, lanes_all), bf16),
        pltpu.VMEM((2, channels, lanes_all), bf16),
        wide, wide, wide, wide,
        pltpu.VMEM((4, tiles, ROWS, LANES), f32),
        pltpu.VMEM((2, tiles, LANES), f32),
        pltpu.VMEM((positions, channels), f32),
        pltpu.VMEM((token_rows, columns), f32),
        pltpu.VMEM((token_rows, n_ep), f32),
        dma((len(given),)),
        dma((n_ep // 2,)), dma((n_ep // 2,)), dma((n_ep // 2,)), dma((n_ep,)), dma((n_ep,)), dma((n_ep,)),
        dma((n_ep + 1,)), dma((n_ep + 1,)), dma((n_ep + 1,)), dma((n_ep + 1,)),
        dma((n_ep,)), dma((n_ep,)), dma((n_ep,)), dma((n_ep,)),
        dma((4,)),
    ]
    return pl.pallas_call(
        functools.partial(body, n_ep, n_tp),
        out_shape=[
            jax.ShapeDtypeStruct((positions, columns), bf16),
            jax.ShapeDtypeStruct((token_rows, columns), bf16),
        ],
        in_specs=[pl.BlockSpec(memory_space=pl.ANY)] * len(given),
        out_specs=[pl.BlockSpec(memory_space=pltpu.VMEM)] * 2,
        scratch_shapes=scratch,
        compiler_params=pltpu.CompilerParams(
            collective_id=0, has_side_effects=True, vmem_limit_bytes=VMEM_BYTES
        ),
        name="both_batches",
    )(*given)


def solution(mesh):
    return jax.shard_map(
        on_device,
        mesh=mesh,
        in_specs=(
            P("ep", "tp"),
            P("tp", "ep"),
            P("tp", "ep"),
            P("tp", None),
            P("tp", None),
            P(None, "tp", None, None),
            P(None, "tp", None, None),
            P("tp"),
            P(),
            P(None, "tp"),
            P("ep", None),
            P(),
            P("ep", None),
            P("ep", None),
            P("ep", None, "tp"),
            P("ep", None, "tp"),
            P("ep", None, "tp"),
            P(None, "tp"),
            P(None, "tp"),
            P(None, "tp"),
        ),
        out_specs=(P("ep", "tp"), P("ep", "tp")),
        check_vma=False,
    )
```

```python
import functools

import jax
import jax.numpy as jnp
from jax import lax
from jax.experimental import pallas as pl
from jax.experimental.pallas import tpu as pltpu
from jax.sharding import PartitionSpec as P

eps_norm = 1e-06
LANES = 128
ROWS = 8
MESH = pl.DeviceIdType.MESH
bf16, f32 = jnp.bfloat16, jnp.float32
EARLY_TILES = 4
VMEM_BYTES = 62 * 1024 * 1024


def cos_sin(angle):
    turns = jnp.floor(angle * 0.6366197723675814 + 0.5)
    rest = ((angle - turns * 1.5703125) - turns * 4.837512969970703125e-4) - turns * 7.549789954891882e-8
    square = rest * rest
    sine = rest + rest * square * (
        -1.6666654611e-1 + square * (8.3321608736e-3 + square * -1.9515295891e-4)
    )
    cosine = (
        1.0
        - 0.5 * square
        + square
        * square
        * (
            4.166664568298827e-2
            + square * (-1.388731625493765e-3 + square * 2.443315711809948e-5)
        )
    )
    quarter = turns.astype(jnp.int32)
    odd = (quarter & 1) == 1
    out_cos = jnp.where(odd, sine, cosine)
    out_sin = jnp.where(odd, cosine, sine)
    out_cos = jnp.where(((quarter + 1) & 2) == 2, -out_cos, out_cos)
    out_sin = jnp.where((quarter & 2) == 2, -out_sin, out_sin)
    return out_cos, out_sin


def one_minus_exp_neg(y):
    series = y * (
        1.0
        - y * (1.0 / 2)
        * (1.0 - y * (1.0 / 3) * (1.0 - y * (1.0 / 4) * (1.0 - y * (1.0 / 5) * (1.0 - y * (1.0 / 6)))))
    )
    return jnp.where(y < 0.3, series, 1.0 - jnp.exp(-y))


def dot(a, b, dims=((1,), (0,)), precision=None):
    return lax.dot_general(a, b, (dims, ((), ())), preferred_element_type=f32, precision=precision)


def iota(shape, axis):
    return lax.broadcasted_iota(jnp.int32, shape, axis)


def ones_where(condition, dtype=bf16):
    return jnp.where(condition, 1.0, 0.0).astype(dtype)


def scaled_rows(values, gain):
    widened = values.astype(f32)
    factor = lax.rsqrt(jnp.mean(widened * widened, axis=-1, keepdims=True) + eps_norm)
    return (widened * factor * gain).astype(bf16)


def body(
    n_ep, n_tp,
    u_hbm, logs_hbm, loss_hbm, eig_hbm, freq_hbm, gin_hbm, gout_hbm, feed_hbm, mscale_hbm, mweight_hbm,
    x_hbm, gain_hbm, routes_hbm, chosen_hbm, gate_hbm, up_hbm, down_hbm, sgate_hbm, sup_hbm, sdown_hbm,
    mixed_hbm, moe_hbm,
    u, logs, loss, eig, freq, gin, gout, feed, mscale, mweight,
    x, gain, routes, chosen, gate, up, down, sgate, sup, sdown,
    tok, hid, res, ret, ends, ssm,
    us, parts, eigrow, freqrow, win, wout, ar_ref, ai_ref, br_ref, bi_ref, pre, inc, total, shared_cols, shares,
    load_sem,
    tok_up, tok_dn, tok_x, tok_sib, tok_recv, tok_recv_sib,
    hid_send_y, hid_send_sib, hid_recv_y, hid_recv_sib,
    res_send, res_recv, ends_send, ends_recv,
    ssm_sem, store_sem, mixed_ref, moe_ref,
):
    e, t = lax.axis_index("ep"), lax.axis_index("tp")
    n_line, n_y = n_ep // 2, n_tp // 2
    a, b = e // 2, e % 2
    y, c = t // 2, t % 2
    steps = n_ep
    token_rows, width = x.shape
    half = width // 2
    hidden = gate.shape[1]
    columns = down.shape[1]
    positions, channels = u.shape
    groups, states = eig.shape
    group_ch = channels // groups
    lanes_all = groups * states
    tiles = lanes_all // LANES
    per_tile = LANES // states
    segment = positions // ROWS

    barrier = pltpu.get_barrier_semaphore()
    for i in range(n_ep):
        @pl.when(e != i)
        def _():
            pl.semaphore_signal(barrier, inc=1, device_id={"ep": i, "tp": t}, device_id_type=MESH)
    for i in range(n_tp):
        @pl.when(t != i)
        def _():
            pl.semaphore_signal(barrier, inc=1, device_id={"ep": e, "tp": i}, device_id_type=MESH)

    pairs = [
        (x_hbm, x), (gain_hbm, gain), (sgate_hbm, sgate), (sup_hbm, sup), (gate_hbm.at[0], gate), (up_hbm.at[0], up),
        (u_hbm, u), (logs_hbm, logs), (loss_hbm, loss), (eig_hbm, eig), (freq_hbm, freq), (gin_hbm, gin),
        (gout_hbm, gout), (feed_hbm, feed), (down_hbm.at[0], down), (sdown_hbm, sdown), (mscale_hbm, mscale),
        (mweight_hbm, mweight), (routes_hbm, routes), (chosen_hbm, chosen),
    ]
    loads = [pltpu.make_async_copy(src, dst, load_sem.at[k]) for k, (src, dst) in enumerate(pairs)]
    for load in loads:
        load.start()

    left, right = a, n_line - 1 - a
    short = jnp.minimum(left, right)
    sign_long = jnp.where(left <= right, 1, -1)

    def near(k):
        odd = k % 2
        alternating = jnp.where(odd == 1, sign_long, -sign_long) * ((k + 1) // 2)
        beyond = sign_long * (k - short)
        return a + jnp.where(k <= 2 * short, alternating, beyond)

    def place(s):
        last = s == steps - 1
        odd = s % 2 == 1
        k = jnp.where(last, n_line - 1, jnp.where(odd, (s + 1) // 2, s // 2 - 1))
        other = jnp.where(last, 1, jnp.where(odd, 0, 1))
        own_first = short >= 1
        swapped = jnp.where(s == n_line, 1, jnp.where(s == n_line + 1, 0, s - n_line))
        k = jnp.where(own_first, jnp.where(s < n_line, s, swapped), k)
        other = jnp.where(own_first, jnp.where(s < n_line, 0, 1), other)
        k = jnp.where(s == 0, 0, k)
        other = jnp.where(s == 0, 0, other)
        row = jnp.where(k == 0, a, near(k))
        return row, other

    def block_of(row, other):
        return row * 2 + jnp.where(other == 1, 1 - b, b)

    def token_copy(blk, half_index, send, recv, ep, tp):
        part = tok.at[blk, :, pl.ds(pl.multiple_of(half_index * half, half), half)]
        return pltpu.make_async_remote_copy(
            part, part, send, recv, device_id={"ep": ep, "tp": tp}, device_id_type=MESH
        )

    sib = y * 2 + 1 - c

    def up_copy(row):
        return token_copy(row * 2 + b, c, tok_up.at[row], tok_recv.at[row * 2 + b], jnp.minimum(e + 2, n_ep - 2 + b), t)

    def dn_copy(row):
        return token_copy(row * 2 + b, c, tok_dn.at[row], tok_recv.at[row * 2 + b], jnp.maximum(e - 2, b), t)

    def x_copy(row):
        return token_copy(row * 2 + b, c, tok_x.at[row], tok_recv.at[row * 2 + b], a * 2 + 1 - b, t)

    def sib_copy(blk):
        return token_copy(blk, c, tok_sib.at[blk], tok_recv_sib.at[blk], e, sib)

    def forward(row):
        @pl.when((row <= a) & (a + 1 < n_line))
        def _():
            up_copy(row).start()

        @pl.when((row >= a) & (a >= 1))
        def _():
            dn_copy(row).start()

        x_copy(row).start()

    def hid_y_copy(s, yy):
        part = hid.at[s, c, y]
        return pltpu.make_async_remote_copy(
            part, part, hid_send_y.at[s], hid_recv_y.at[s], device_id={"ep": e, "tp": yy * 2 + c}, device_id_type=MESH
        )

    def hid_sib_copy(s, yy):
        part = hid.at[s, c, yy]
        return pltpu.make_async_remote_copy(
            part, part, hid_send_sib.at[s], hid_recv_sib.at[s], device_id={"ep": e, "tp": sib}, device_id_type=MESH
        )

    def span(ref, send, recv):
        return pltpu.make_async_remote_copy(
            ref, ref, send, recv, device_id={"ep": e, "tp": sib}, device_id_type=MESH
        )

    def gated(rows, gate_w, up_w, s):
        block = min(256, hidden)
        for n in range(hidden // block):
            cols = pl.ds(n * block, block)
            gate_part = dot(rows, gate_w[:, cols])
            up_part = dot(rows, up_w[:, cols])
            hid[s, c, y, :, cols] = (gate_part / (1.0 + jnp.exp(-gate_part)) * up_part).astype(bf16)

    def send_hidden(s):
        for dy in range(1, n_y):
            hid_y_copy(s, lax.rem(y + dy, n_y)).start()
        hid_sib_copy(s, y).start()

    def relay_hidden(s):
        span(hid.at[s, c, pl.ds(0, n_y - 1)], hid_send_y.at[s], hid_recv_y.at[s]).wait_recv()
        for dy in range(1, n_y):
            hid_sib_copy(s, lax.rem(y + dy, n_y)).start()

    def down_product(s, weight):
        span(hid.at[s, 1 - c], hid_send_sib.at[s], hid_recv_sib.at[s]).wait_recv()
        value = None
        for cc in range(2):
            for yy in range(n_y):
                rows = (yy * 2 + cc) * hidden
                term = dot(hid[s, cc, yy], weight[rows : rows + hidden, :])
                value = term if value is None else value + term
        return value

    def res_copy(blk):
        return pltpu.make_async_remote_copy(
            res.at[blk], ret.at[e], res_send.at[blk], res_recv.at[e], device_id={"ep": blk, "tp": t}, device_id_type=MESH
        )

    loads[0].wait()
    loads[1].wait()
    tok[e] = scaled_rows(x[...], gain[...])
    pl.semaphore_wait(barrier, n_ep + n_tp - 2)
    forward(a)

    loads[2].wait()
    loads[3].wait()
    gated(tok[e], sgate, sup, steps)
    send_hidden(steps)
    loads[4].wait()
    loads[5].wait()
    gated(tok[e], gate, up, 0)
    send_hidden(0)

    for k in range(6, 14):
        loads[k].wait()
    shuffle = ones_where(iota((positions, positions), 1) == (iota((positions, positions), 0) % ROWS) * segment + iota((positions, positions), 0) // ROWS)
    us[...] = dot(shuffle, u[...]).astype(bf16)
    parts[...] = jnp.zeros(parts.shape, bf16)
    slot = parts.shape[1] // 3
    for q, table in enumerate((jnp.exp(logs[...]), loss[...])):
        rest = table
        for r in range(3):
            piece = rest.astype(bf16)
            rest = rest - piece.astype(f32)
            parts[q, r * slot : r * slot + groups, :] = dot(piece, shuffle, ((1,), (1,))).astype(bf16)
    spread = ones_where(iota((states, LANES), 1) % states == iota((states, LANES), 0), f32)
    for table, rows_ref in ((eig, eigrow), (freq, freqrow)):
        wide = dot(table[...], spread, precision=lax.Precision.HIGHEST)
        row = jnp.zeros((tiles, LANES), f32)
        for h in range(per_tile):
            pick = ones_where(iota((tiles, groups), 1) == iota((tiles, groups), 0) * per_tile + h, f32)
            picked = dot(pick, wide, precision=lax.Precision.HIGHEST)
            row = jnp.where(iota((tiles, LANES), 1) // states == h, picked, row)
        rows_ref[...] = row
    spread_all = ones_where(iota((states, lanes_all), 1) % states == iota((states, lanes_all), 0))
    own_group = iota((channels, lanes_all), 0) // group_ch == iota((channels, lanes_all), 1) // states
    for r in range(2):
        win[r] = jnp.where(own_group, dot(gin[r], spread_all), 0.0).astype(bf16)
        wout[r] = jnp.where(own_group, dot(gout[r], spread_all), 0.0).astype(bf16)

    def tile_work(i):
        lanes = pl.ds(pl.multiple_of(i * LANES, LANES), LANES)
        slot_rows = 3 * slot
        own = iota((slot_rows, LANES), 0) % slot == per_tile * i + iota((slot_rows, LANES), 1) // states
        select = ones_where(own)
        step_wide = dot(parts[0], select, ((0,), (0,)))
        loss_wide = dot(parts[1], select, ((0,), (0,)))
        loss_rate = eigrow[pl.ds(i, 1), :] * step_wide
        magnitude = jnp.exp(loss_wide - loss_rate)
        cosine, sine = cos_sin(freqrow[pl.ds(i, 1), :] * step_wide)
        scaling = jnp.sqrt(one_minus_exp_neg(2.0 * loss_rate))
        ar_ref[:, lanes] = magnitude * cosine
        ai_ref[:, lanes] = magnitude * sine
        br_ref[:, lanes] = scaling * dot(us[...], win[0, :, lanes])
        bi_ref[:, lanes] = scaling * dot(us[...], win[1, :, lanes])
        reach = jnp.ones((ROWS, LANES), f32), jnp.zeros((ROWS, LANES), f32)
        state = jnp.zeros((ROWS, LANES), f32), jnp.zeros((ROWS, LANES), f32)
        for j in range(segment):
            at = pl.ds(j * ROWS, ROWS)
            ar, ai, br, bi = ar_ref[at, lanes], ai_ref[at, lanes], br_ref[at, lanes], bi_ref[at, lanes]
            reach = ar * reach[0] - ai * reach[1], ar * reach[1] + ai * reach[0]
            state = ar * state[0] - ai * state[1] + br, ar * state[1] + ai * state[0] + bi
            ar_ref[at, lanes] = reach[0]
            ai_ref[at, lanes] = reach[1]
            br_ref[at, lanes] = state[0]
            bi_ref[at, lanes] = state[1]
        row = iota((ROWS, LANES), 0)
        er, ei = jnp.ones((1, LANES), f32), jnp.zeros((1, LANES), f32)
        sr, si = jnp.zeros((1, LANES), f32), jnp.zeros((1, LANES), f32)
        pre_r = pre_i = pre_sr = pre_si = jnp.zeros((ROWS, LANES), f32)
        for k in range(ROWS):
            here = row == k
            pre_r = jnp.where(here, er, pre_r)
            pre_i = jnp.where(here, ei, pre_i)
            pre_sr = jnp.where(here, sr, pre_sr)
            pre_si = jnp.where(here, si, pre_si)
            tr, ti = reach[0][k : k + 1], reach[1][k : k + 1]
            ur, ui = state[0][k : k + 1], state[1][k : k + 1]
            er, ei, sr, si = (
                tr * er - ti * ei,
                tr * ei + ti * er,
                tr * sr - ti * si + ur,
                tr * si + ti * sr + ui,
            )
        for q, value in enumerate((pre_r, pre_i, pre_sr, pre_si)):
            pre[q, i] = value
        for q, value in enumerate((er, ei, sr, si)):
            ends[e, q, pl.ds(i, 1), :] = value

    def ends_copy(i):
        return pltpu.make_async_remote_copy(
            ends.at[e], ends.at[e], ends_send.at[i], ends_recv.at[e], device_id={"ep": i, "tp": t}, device_id_type=MESH
        )

    def send_ends():
        for i in range(1, n_ep):
            @pl.when(i > e)
            def _():
                ends_copy(i).start()

    def incoming():
        zero = jnp.zeros((tiles, LANES), f32)
        inc[0] = zero
        inc[1] = zero
        for i in range(n_ep - 1):
            @pl.when(i < e)
            def _():
                part = ends.at[i]
                pltpu.make_async_remote_copy(
                    part, part, ends_send.at[i], ends_recv.at[i], device_id={"ep": e, "tp": sib}, device_id_type=MESH
                ).wait_recv()
                tr, ti, ur, ui = ends[i, 0], ends[i, 1], ends[i, 2], ends[i, 3]
                sr, si = inc[0], inc[1]
                inc[0] = tr * sr - ti * si + ur
                inc[1] = tr * si + ti * sr + ui

    def split(value):
        high = value.astype(bf16)
        return high, (value - high.astype(f32)).astype(bf16)

    def read_tile(i):
        lanes = pl.ds(pl.multiple_of(i * LANES, LANES), LANES)
        ir, ii = inc[0, pl.ds(i, 1), :], inc[1, pl.ds(i, 1), :]
        pre_r, pre_i, pre_sr, pre_si = pre[0, i], pre[1, i], pre[2, i], pre[3, i]
        enter_r = (pre_sr + pre_r * ir - pre_i * ii)[None]
        enter_i = (pre_si + pre_r * ii + pre_i * ir)[None]
        shape = (segment, ROWS, LANES)
        ar, ai = ar_ref[:, lanes].reshape(shape), ai_ref[:, lanes].reshape(shape)
        br, bi = br_ref[:, lanes].reshape(shape), bi_ref[:, lanes].reshape(shape)
        state_r = (br + ar * enter_r - ai * enter_i).reshape(positions, LANES)
        state_i = (bi + ar * enter_i + ai * enter_r).reshape(positions, LANES)
        wr, wi = wout[0, :, lanes], -wout[1, :, lanes]
        high_r, low_r = split(state_r)
        high_i, low_i = split(state_i)
        nt = ((1,), (1,))
        total[...] += (dot(high_r, wr, nt) + dot(low_r, wr, nt)) + (dot(high_i, wi, nt) + dot(low_i, wi, nt))

    def ssm_y_copy(yy):
        part = ssm.at[c, y]
        return pltpu.make_async_remote_copy(
            part, part, ssm_sem.at[0], ssm_sem.at[1], device_id={"ep": e, "tp": yy * 2 + c}, device_id_type=MESH
        )

    def ssm_sib_copy(yy):
        part = ssm.at[c, yy]
        return pltpu.make_async_remote_copy(
            part, part, ssm_sem.at[2], ssm_sem.at[3], device_id={"ep": e, "tp": sib}, device_id_type=MESH
        )

    def read_out():
        total[...] = feed[...] * us[...].astype(f32)
        lax.fori_loop(0, tiles, lambda i, _: (read_tile(i), 0)[1], 0)
        value = total[...]
        inner = 0.7978845608028654 * (value + 0.044715 * (value * value * value))
        result = (0.5 * value * (1.0 + jnp.tanh(inner))).astype(bf16)
        unshuffle = ones_where(iota((positions, positions), 1) == (iota((positions, positions), 0) % segment) * ROWS + iota((positions, positions), 0) // segment)
        ssm[c, y] = dot(unshuffle, result).astype(bf16)
        for dy in range(1, n_y):
            ssm_y_copy(lax.rem(y + dy, n_y)).start()
        ssm_sib_copy(y).start()

    for k in range(14, 20):
        loads[k].wait()

    early = min(EARLY_TILES, tiles)
    lax.fori_loop(0, early, lambda i, _: (tile_work(i), 0)[1], 0)

    def arrive(s):
        row, other = place(s)
        blk = block_of(row, other)
        token_copy(blk, c, tok_sib.at[blk], tok_recv.at[blk], e, sib).wait_recv()

        @pl.when(other == 0)
        def _():
            forward(row)

        sib_copy(blk).start()

    def first_products(s):
        row, other = place(s)
        blk = block_of(row, other)
        token_copy(blk, 1 - c, tok_sib.at[blk], tok_recv_sib.at[blk], e, sib).wait_recv()
        gated(tok[blk], gate, up, s)
        send_hidden(s)

    def held(s):
        return (s == 2) & (short < 1) & (steps >= 6)

    def last_product(s):
        row, other = place(s)
        blk = block_of(row, other)
        value = down_product(s, down).astype(bf16)

        @pl.when(blk == e)
        def _():
            ret[e] = value

        @pl.when(blk != e)
        def _():
            res[blk] = value

        @pl.when((blk != e) & jnp.logical_not(held(s)))
        def _():
            res_copy(blk).start()

    last_pair = steps // 2

    def one(q, act):
        @pl.when((q >= 0) & (q < steps))
        def _():
            act(q)

    def pair(p, carry):
        one(2 * p - 1, arrive)
        one(2 * p, arrive)

        @pl.when((p == 3) & (short < 1) & (steps >= 6))
        def _():
            row, other = place(2)
            res_copy(block_of(row, other)).start()

        one(2 * p - 1, first_products)

        @pl.when(p != last_pair)
        def _():
            one(2 * p - 3, relay_hidden)

        @pl.when(p == last_pair)
        def _():
            one(2 * p - 3, last_product)

        one(2 * p, first_products)
        one(2 * p - 2, relay_hidden)

        @pl.when(p == 1)
        def _():
            relay_hidden(steps)

        @pl.when(p <= 2)
        def _():
            middle = (early + tiles) // 2
            lax.fori_loop(jnp.where(p == 1, early, middle), jnp.where(p == 1, middle, tiles), lambda i, _: (tile_work(i), 0)[1], 0)

        @pl.when(p == 2)
        def _():
            send_ends()

        @pl.when(p != last_pair)
        def _():
            one(2 * p - 3, last_product)

        one(2 * p - 2, last_product)

        @pl.when(p == last_pair - 1)
        def _():
            incoming()
            read_out()
            one(2 * p - 1, relay_hidden)

        @pl.when(p == last_pair)
        def _():
            span(ssm.at[c, pl.ds(0, n_y - 1)], ssm_sem.at[0], ssm_sem.at[1]).wait_recv()
            for dy in range(1, n_y):
                ssm_sib_copy(lax.rem(y + dy, n_y)).start()
            shared_cols[...] = down_product(steps, sdown)

        return carry

    lax.fori_loop(1, steps // 2 + 2, pair, 0)

    span(ssm.at[1 - c], ssm_sem.at[2], ssm_sem.at[3]).wait_recv()
    squares = jnp.zeros((positions, 1), f32)
    for cc in range(2):
        for yy in range(n_y):
            piece = ssm[cc, yy].astype(f32)
            squares = squares + jnp.sum(piece * piece, axis=-1, keepdims=True)
    factor = lax.rsqrt(squares / (channels * n_tp) + eps_norm)

    def gain_of(tt):
        if channels % LANES == 0:
            return mscale[:, tt * channels : (tt + 1) * channels]
        return mscale[tt : tt + 1, :]

    value = None
    for cc in range(2):
        for yy in range(n_y):
            tt = yy * 2 + cc
            normed = (ssm[cc, yy].astype(f32) * factor * gain_of(tt)).astype(bf16)
            term = dot(normed, mweight[tt * channels : (tt + 1) * channels, :])
            value = term if value is None else value + term
    mixed_ref[...] = value.astype(bf16)
    mixed_store = pltpu.make_async_copy(mixed_ref, mixed_hbm, store_sem.at[0])
    mixed_store.start()

    taken = jnp.zeros((n_ep, token_rows), f32)
    for k in range(routes.shape[0]):
        taken = taken + jnp.where(iota((n_ep, token_rows), 0) == routes[k : k + 1, :], chosen[k : k + 1, :], 0.0)
    shares[...] = taken.T

    def combine(s, carry):
        row, other = place(s)
        i = block_of(row, other)

        @pl.when(i != e)
        def _():
            part = ret.at[i]
            pltpu.make_async_remote_copy(
                part, part, res_send.at[i], res_recv.at[i], device_id={"ep": e, "tp": sib}, device_id_type=MESH
            ).wait_recv()

        share = jnp.sum(jnp.where(iota((token_rows, n_ep), 1) == i, shares[...], 0.0), axis=1, keepdims=True)
        shared_cols[...] += ret[i].astype(f32) * share
        return carry

    lax.fori_loop(0, steps, combine, 0)
    moe_ref[...] = shared_cols[...].astype(bf16)
    moe_store = pltpu.make_async_copy(moe_ref, moe_hbm, store_sem.at[1])
    moe_store.start()

    def drain(s, carry):
        @pl.when(s != e)
        def _():
            token_copy(s, c, tok_sib.at[s], tok_recv_sib.at[s], e, sib).wait_send()
            res_copy(s).wait_send()

        @pl.when(s > e)
        def _():
            ends_copy(s).wait_send()

        return carry

    lax.fori_loop(0, n_ep, drain, 0)

    def drain_line(row, carry):
        @pl.when((row <= a) & (a + 1 < n_line))
        def _():
            up_copy(row).wait_send()

        @pl.when((row >= a) & (a >= 1))
        def _():
            dn_copy(row).wait_send()

        x_copy(row).wait_send()
        return carry

    lax.fori_loop(0, n_line, drain_line, 0)

    def drain_hidden(s, carry):
        span(hid.at[s, c, pl.ds(0, n_y - 1)], hid_send_y.at[s], hid_recv_y.at[s]).wait_send()
        span(hid.at[s, c], hid_send_sib.at[s], hid_recv_sib.at[s]).wait_send()
        return carry

    lax.fori_loop(0, steps + 1, drain_hidden, 0)
    span(ssm.at[c, pl.ds(0, n_y - 1)], ssm_sem.at[0], ssm_sem.at[1]).wait_send()
    span(ssm.at[c], ssm_sem.at[2], ssm_sem.at[3]).wait_send()
    mixed_store.wait()
    moe_store.wait()


def hand_over(mixed, moe_out):
    def copy(mixed_in, moe_in, mixed_ref, moe_ref):
        mixed_ref[...] = mixed_in[...]
        moe_ref[...] = moe_in[...]

    specs = [pl.BlockSpec(v.shape, lambda i: (0, 0)) for v in (mixed, moe_out)]
    return pl.pallas_call(
        copy,
        grid=(1,),
        in_specs=specs,
        out_specs=specs,
        out_shape=[jax.ShapeDtypeStruct(v.shape, v.dtype) for v in (mixed, moe_out)],
        name="hand_over",
    )(mixed, moe_out)


def on_device(*operands):
    (
        u, logs, losses, eigen, frequency, group_in, group_out, feed, mixer_scale, mixer_weight,
        x, gain, routes, chosen, gate, up, down, shared_gate, shared_up, shared_down,
    ) = operands
    n_ep, n_tp = lax.axis_size("ep"), lax.axis_size("tp")
    positions, channels = u.shape
    groups, states = eigen.shape
    lanes_all = groups * states
    tiles = lanes_all // LANES
    token_rows, width = x.shape
    hidden, columns = gate.shape[2], down.shape[2]
    group_in = group_in.transpose(0, 1, 3, 2).reshape(2, channels, states)
    group_out = group_out.reshape(2, channels, states)
    feed = feed.reshape(1, channels)
    mixer_scale = mixer_scale.reshape((1, -1) if channels % LANES == 0 else (n_tp, channels))
    gain = gain.reshape(1, width)
    routes, chosen = routes.T, chosen.T
    given = (
        u, logs, losses, eigen, frequency, group_in, group_out, feed, mixer_scale, mixer_weight,
        x, gain, routes, chosen, gate, up, down, shared_gate, shared_up, shared_down,
    )
    local = [
        pltpu.VMEM(g.shape[1:] if k in (14, 15, 16) else g.shape, g.dtype) for k, g in enumerate(given)
    ]
    slot = -(-groups // 16) * 16
    wide = pltpu.VMEM((positions, lanes_all), f32)
    dma = pltpu.SemaphoreType.DMA
    scratch = local + [
        pltpu.VMEM((n_ep, token_rows, width), bf16),
        pltpu.VMEM((n_ep + 1, 2, n_tp // 2, token_rows, hidden), bf16),
        pltpu.VMEM((n_ep, token_rows, columns), bf16),
        pltpu.VMEM((n_ep, token_rows, columns), bf16),
        pltpu.VMEM((n_ep, 4, tiles, LANES), f32),
        pltpu.VMEM((2, n_tp // 2, positions, channels), bf16),
        pltpu.VMEM((positions, channels), bf16),
        pltpu.VMEM((2, 3 * slot, positions), bf16),
        pltpu.VMEM((tiles, LANES), f32),
        pltpu.VMEM((tiles, LANES), f32),
        pltpu.VMEM((2, channels, lanes_all), bf16),
        pltpu.VMEM((2, channels, lanes_all), bf16),
        wide, wide, wide, wide,
        pltpu.VMEM((4, tiles, ROWS, LANES), f32),
        pltpu.VMEM((2, tiles, LANES), f32),
        pltpu.VMEM((positions, channels), f32),
        pltpu.VMEM((token_rows, columns), f32),
        pltpu.VMEM((token_rows, n_ep), f32),
        dma((len(given),)),
        dma((n_ep // 2,)), dma((n_ep // 2,)), dma((n_ep // 2,)), dma((n_ep,)), dma((n_ep,)), dma((n_ep,)),
        dma((n_ep + 1,)), dma((n_ep + 1,)), dma((n_ep + 1,)), dma((n_ep + 1,)),
        dma((n_ep,)), dma((n_ep,)), dma((n_ep,)), dma((n_ep,)),
        dma((4,)),
        dma((2,)),
        pltpu.VMEM((positions, columns), bf16),
        pltpu.VMEM((token_rows, columns), bf16),
    ]
    mixed, moe_out = pl.pallas_call(
        functools.partial(body, n_ep, n_tp),
        out_shape=[
            jax.ShapeDtypeStruct((positions, columns), bf16),
            jax.ShapeDtypeStruct((token_rows, columns), bf16),
        ],
        in_specs=[pl.BlockSpec(memory_space=pl.ANY)] * len(given),
        out_specs=[pl.BlockSpec(memory_space=pl.ANY)] * 2,
        scratch_shapes=scratch,
        compiler_params=pltpu.CompilerParams(
            collective_id=0, has_side_effects=True, vmem_limit_bytes=VMEM_BYTES
        ),
        name="both_batches",
    )(*given)
    return hand_over(mixed, moe_out)


def solution(mesh):
    return jax.shard_map(
        on_device,
        mesh=mesh,
        in_specs=(
            P("ep", "tp"),
            P("tp", "ep"),
            P("tp", "ep"),
            P("tp", None),
            P("tp", None),
            P(None, "tp", None, None),
            P(None, "tp", None, None),
            P("tp"),
            P(),
            P(None, "tp"),
            P("ep", None),
            P(),
            P("ep", None),
            P("ep", None),
            P("ep", None, "tp"),
            P("ep", None, "tp"),
            P("ep", None, "tp"),
            P(None, "tp"),
            P(None, "tp"),
            P(None, "tp"),
        ),
        out_specs=(P("ep", "tp"), P("ep", "tp")),
        check_vma=False,
    )
```

```python
import functools

import jax
import jax.numpy as jnp
from jax import lax
from jax.experimental import pallas as pl
from jax.experimental.pallas import tpu as pltpu
from jax.sharding import PartitionSpec as P

eps_norm = 1e-06
LANES = 128
ROWS = 8
MESH = pl.DeviceIdType.MESH
bf16, f32 = jnp.bfloat16, jnp.float32
PIECES = 2
TILES_IN_FIRST = 6
VMEM_BYTES = 62 * 1024 * 1024


def cos_sin(angle):
    turns = jnp.floor(angle * 0.6366197723675814 + 0.5)
    rest = ((angle - turns * 1.5703125) - turns * 4.837512969970703125e-4) - turns * 7.549789954891882e-8
    square = rest * rest
    sine = rest + rest * square * (
        -1.6666654611e-1 + square * (8.3321608736e-3 + square * -1.9515295891e-4)
    )
    cosine = (
        1.0
        - 0.5 * square
        + square
        * square
        * (
            4.166664568298827e-2
            + square * (-1.388731625493765e-3 + square * 2.443315711809948e-5)
        )
    )
    quarter = turns.astype(jnp.int32)
    odd = (quarter & 1) == 1
    out_cos = jnp.where(odd, sine, cosine)
    out_sin = jnp.where(odd, cosine, sine)
    out_cos = jnp.where(((quarter + 1) & 2) == 2, -out_cos, out_cos)
    out_sin = jnp.where((quarter & 2) == 2, -out_sin, out_sin)
    return out_cos, out_sin


def one_minus_exp_neg(y):
    series = y * (
        1.0
        - y * (1.0 / 2)
        * (1.0 - y * (1.0 / 3) * (1.0 - y * (1.0 / 4) * (1.0 - y * (1.0 / 5) * (1.0 - y * (1.0 / 6)))))
    )
    return jnp.where(y < 0.3, series, 1.0 - jnp.exp(-y))


def dot(a, b, dims=((1,), (0,)), precision=None):
    return lax.dot_general(a, b, (dims, ((), ())), preferred_element_type=f32, precision=precision)


def iota(shape, axis):
    return lax.broadcasted_iota(jnp.int32, shape, axis)


def ones_where(condition, dtype=bf16):
    return jnp.where(condition, 1.0, 0.0).astype(dtype)


def scaled_rows(values, gain):
    widened = values.astype(f32)
    factor = lax.rsqrt(jnp.mean(widened * widened, axis=-1, keepdims=True) + eps_norm)
    return (widened * factor * gain).astype(bf16)


def body(
    n_ep, n_tp,
    u_hbm, logs_hbm, loss_hbm, eig_hbm, freq_hbm, gin_hbm, gout_hbm, feed_hbm, mscale_hbm, mweight_hbm,
    x_hbm, gain_hbm, routes_hbm, chosen_hbm, gate_hbm, up_hbm, down_hbm, sgate_hbm, sup_hbm, sdown_hbm,
    mixed_hbm, sum_hbm, late_hbm, weight_hbm,
    u, logs, loss, eig, freq, gin, gout, feed, mscale, mweight,
    x, gain, routes, chosen, gate, up, down, sgate, sup, sdown,
    tok, hid, res, ret, ends, ssm,
    us, parts, eigrow, freqrow, win, wout, ar_ref, ai_ref, br_ref, bi_ref, whole, pre, inc, total, shared_cols, shares,
    load_sem,
    tok_up, tok_dn, tok_x, tok_sib, tok_recv, tok_recv_sib,
    hid_send_y, hid_send_sib, hid_recv_y, hid_recv_sib,
    res_send, res_recv, ends_send, ends_recv,
    ssm_sem, store_sem, mixed_ref, late_weight,
):
    e, t = lax.axis_index("ep"), lax.axis_index("tp")
    n_line, n_y = n_ep // 2, n_tp // 2
    a, b = e // 2, e % 2
    y, c = t // 2, t % 2
    steps = n_ep
    token_rows, width = x.shape
    half = width // 2
    hidden = gate.shape[1]
    columns = down.shape[1]
    positions, channels = u.shape
    groups, states = eig.shape
    group_ch = channels // groups
    lanes_all = groups * states
    tiles = lanes_all // LANES
    per_tile = LANES // states
    segment = positions // ROWS

    barrier = pltpu.get_barrier_semaphore()
    for i in range(n_ep):
        @pl.when(e != i)
        def _():
            pl.semaphore_signal(barrier, inc=1, device_id={"ep": i, "tp": t}, device_id_type=MESH)
    for i in range(n_tp):
        @pl.when(t != i)
        def _():
            pl.semaphore_signal(barrier, inc=1, device_id={"ep": e, "tp": i}, device_id_type=MESH)

    pairs = [
        (x_hbm, x), (gain_hbm, gain), (sgate_hbm, sgate), (sup_hbm, sup), (gate_hbm.at[0], gate), (up_hbm.at[0], up),
        (u_hbm, u), (logs_hbm, logs), (loss_hbm, loss), (eig_hbm, eig), (freq_hbm, freq), (gin_hbm, gin),
        (gout_hbm, gout), (feed_hbm, feed), (down_hbm.at[0], down), (sdown_hbm, sdown), (mscale_hbm, mscale),
        (mweight_hbm, mweight), (routes_hbm, routes), (chosen_hbm, chosen),
    ]
    loads = [pltpu.make_async_copy(src, dst, load_sem.at[k]) for k, (src, dst) in enumerate(pairs)]
    for load in loads:
        load.start()

    left, right = a, n_line - 1 - a
    short = jnp.minimum(left, right)
    sign_long = jnp.where(left <= right, 1, -1)

    def near(k):
        odd = k % 2
        alternating = jnp.where(odd == 1, sign_long, -sign_long) * ((k + 1) // 2)
        beyond = sign_long * (k - short)
        return a + jnp.where(k <= 2 * short, alternating, beyond)

    def place(s):
        last = s == steps - 1
        odd = s % 2 == 1
        k = jnp.where(last, n_line - 1, jnp.where(odd, (s + 1) // 2, s // 2 - 1))
        other = jnp.where(last, 1, jnp.where(odd, 0, 1))
        own_first = short >= 1
        swapped = jnp.where(s == n_line, 1, jnp.where(s == n_line + 1, 0, s - n_line))
        k = jnp.where(own_first, jnp.where(s < n_line, s, swapped), k)
        other = jnp.where(own_first, jnp.where(s < n_line, 0, 1), other)
        k = jnp.where(s == 0, 0, k)
        other = jnp.where(s == 0, 0, other)
        row = jnp.where(k == 0, a, near(k))
        return row, other

    def block_of(row, other):
        return row * 2 + jnp.where(other == 1, 1 - b, b)

    piece_rows = token_rows // PIECES

    def token_copy(blk, piece, half_index, send, recv, ep, tp):
        rows = pl.ds(pl.multiple_of(piece * piece_rows, piece_rows), piece_rows)
        part = tok.at[blk, rows, pl.ds(pl.multiple_of(half_index * half, half), half)]
        return pltpu.make_async_remote_copy(
            part, part, send, recv, device_id={"ep": ep, "tp": tp}, device_id_type=MESH
        )

    sib = y * 2 + 1 - c

    def line_copy(row, piece, sent, ep):
        blk = row * 2 + b
        return token_copy(blk, piece, c, sent.at[row, piece], tok_recv.at[blk, piece], ep, t)

    def up_copy(row, piece):
        return line_copy(row, piece, tok_up, jnp.minimum(e + 2, n_ep - 2 + b))

    def dn_copy(row, piece):
        return line_copy(row, piece, tok_dn, jnp.maximum(e - 2, b))

    def x_copy(row, piece):
        return line_copy(row, piece, tok_x, a * 2 + 1 - b)

    def sib_copy(blk, piece):
        return token_copy(blk, piece, c, tok_sib.at[blk, piece], tok_recv_sib.at[blk, piece], e, sib)

    def forward(row, piece):
        @pl.when((row <= a) & (a + 1 < n_line))
        def _():
            up_copy(row, piece).start()

        @pl.when((row >= a) & (a >= 1))
        def _():
            dn_copy(row, piece).start()

        x_copy(row, piece).start()

    def piece_of(piece):
        return pl.ds(piece * piece_rows, piece_rows)

    def hid_y_copy(s, piece, yy):
        part = hid.at[s, c, y, piece_of(piece)]
        return pltpu.make_async_remote_copy(
            part, part, hid_send_y.at[s, piece], hid_recv_y.at[s, piece],
            device_id={"ep": e, "tp": yy * 2 + c}, device_id_type=MESH,
        )

    def hid_sib_copy(s, piece, yy):
        part = hid.at[s, c, yy, piece_of(piece)]
        return pltpu.make_async_remote_copy(
            part, part, hid_send_sib.at[s, piece], hid_recv_sib.at[s, piece],
            device_id={"ep": e, "tp": sib}, device_id_type=MESH,
        )

    def span(ref, send, recv):
        return pltpu.make_async_remote_copy(
            ref, ref, send, recv, device_id={"ep": e, "tp": sib}, device_id_type=MESH
        )

    def from_y(s, piece):
        ref = hid.at[s, c, pl.ds(0, n_y - 1), piece_of(piece)]
        return span(ref, hid_send_y.at[s, piece], hid_recv_y.at[s, piece])

    def from_sib(s, piece, core):
        return span(hid.at[s, core, :, piece_of(piece)], hid_send_sib.at[s, piece], hid_recv_sib.at[s, piece])

    def gated(rows, gate_w, up_w, targets):
        block = min(256, hidden)
        for n in range(hidden // block):
            cols = pl.ds(n * block, block)
            gate_part = dot(rows, gate_w[:, cols])
            up_part = dot(rows, up_w[:, cols])
            value = (gate_part / (1.0 + jnp.exp(-gate_part)) * up_part).astype(bf16)
            done = 0
            for s, into in targets:
                hid[s, c, y, into, cols] = value[done : done + into.size]
                done += into.size

    def send_hidden(s, piece):
        for dy in range(1, n_y):
            hid_y_copy(s, piece, lax.rem(y + dy, n_y)).start()
        hid_sib_copy(s, piece, y).start()

    def relay_hidden(s):
        for piece in range(PIECES):
            from_y(s, piece).wait_recv()
            for dy in range(1, n_y):
                hid_sib_copy(s, piece, lax.rem(y + dy, n_y)).start()

    def down_product(s, weight):
        for piece in range(PIECES):
            from_sib(s, piece, 1 - c).wait_recv()
        value = None
        for cc in range(2):
            for yy in range(n_y):
                rows = (yy * 2 + cc) * hidden
                term = dot(hid[s, cc, yy], weight[rows : rows + hidden, :])
                value = term if value is None else value + term
        return value

    late_target = lax.rem(a + n_line // 2, n_line) * 2 + 1 - b
    late_source = lax.rem(a + n_line - n_line // 2, n_line) * 2 + 1 - b

    def res_copy(blk, into):
        return pltpu.make_async_remote_copy(
            res.at[blk], into, res_send.at[blk], res_recv.at[e], device_id={"ep": blk, "tp": t}, device_id_type=MESH
        )

    def send_result(blk):
        @pl.when(blk == late_target)
        def _():
            res_copy(blk, late_hbm).start()

        @pl.when(blk != late_target)
        def _():
            res_copy(blk, ret.at[e]).start()

    def from_expert(i, into):
        return pltpu.make_async_remote_copy(
            into, into, res_send.at[i], res_recv.at[i], device_id={"ep": e, "tp": sib}, device_id_type=MESH
        )

    loads[0].wait()
    loads[1].wait()
    tok[e] = scaled_rows(x[...], gain[...])
    pl.semaphore_wait(barrier, n_ep + n_tp - 2)
    for piece in range(PIECES):
        forward(a, piece)

    loads[2].wait()
    loads[3].wait()
    everything = pl.ds(0, token_rows)
    gated(tok[e], sgate, sup, [(steps, everything)])
    for piece in range(PIECES):
        send_hidden(steps, piece)
    loads[4].wait()
    loads[5].wait()
    gated(tok[e], gate, up, [(0, everything)])
    for piece in range(PIECES):
        send_hidden(0, piece)

    for k in range(6, 14):
        loads[k].wait()
    shuffle = ones_where(iota((positions, positions), 1) == (iota((positions, positions), 0) % ROWS) * segment + iota((positions, positions), 0) // ROWS)
    us[...] = dot(shuffle, u[...]).astype(bf16)
    parts[...] = jnp.zeros(parts.shape, bf16)
    slot = parts.shape[1] // 3
    for q, table in enumerate((jnp.exp(logs[...]), loss[...])):
        rest = table
        for r in range(3):
            piece = rest.astype(bf16)
            rest = rest - piece.astype(f32)
            parts[q, r * slot : r * slot + groups, :] = dot(piece, shuffle, ((1,), (1,))).astype(bf16)
    spread = ones_where(iota((states, LANES), 1) % states == iota((states, LANES), 0), f32)
    for table, rows_ref in ((eig, eigrow), (freq, freqrow)):
        wide = dot(table[...], spread, precision=lax.Precision.HIGHEST)
        row = jnp.zeros((tiles, LANES), f32)
        for h in range(per_tile):
            pick = ones_where(iota((tiles, groups), 1) == iota((tiles, groups), 0) * per_tile + h, f32)
            picked = dot(pick, wide, precision=lax.Precision.HIGHEST)
            row = jnp.where(iota((tiles, LANES), 1) // states == h, picked, row)
        rows_ref[...] = row
    spread_all = ones_where(iota((states, lanes_all), 1) % states == iota((states, lanes_all), 0))
    own_group = iota((channels, lanes_all), 0) // group_ch == iota((channels, lanes_all), 1) // states
    for r in range(2):
        win[r] = jnp.where(own_group, dot(gin[r], spread_all), 0.0).astype(bf16)
        wout[r] = jnp.where(own_group, dot(gout[r], spread_all), 0.0).astype(bf16)

    def tile_work(i):
        lanes = pl.ds(pl.multiple_of(i * LANES, LANES), LANES)
        slot_rows = 3 * slot
        own = iota((slot_rows, LANES), 0) % slot == per_tile * i + iota((slot_rows, LANES), 1) // states
        select = ones_where(own)
        step_wide = dot(parts[0], select, ((0,), (0,)))
        loss_wide = dot(parts[1], select, ((0,), (0,)))
        loss_rate = eigrow[pl.ds(i, 1), :] * step_wide
        magnitude = jnp.exp(loss_wide - loss_rate)
        cosine, sine = cos_sin(freqrow[pl.ds(i, 1), :] * step_wide)
        scaling = jnp.sqrt(one_minus_exp_neg(2.0 * loss_rate))
        ar_ref[:, lanes] = magnitude * cosine
        ai_ref[:, lanes] = magnitude * sine
        br_ref[:, lanes] = scaling * dot(us[...], win[0, :, lanes])
        bi_ref[:, lanes] = scaling * dot(us[...], win[1, :, lanes])
        reach = jnp.ones((ROWS, LANES), f32), jnp.zeros((ROWS, LANES), f32)
        state = jnp.zeros((ROWS, LANES), f32), jnp.zeros((ROWS, LANES), f32)
        for j in range(segment):
            at = pl.ds(j * ROWS, ROWS)
            ar, ai, br, bi = ar_ref[at, lanes], ai_ref[at, lanes], br_ref[at, lanes], bi_ref[at, lanes]
            reach = ar * reach[0] - ai * reach[1], ar * reach[1] + ai * reach[0]
            state = ar * state[0] - ai * state[1] + br, ar * state[1] + ai * state[0] + bi
            ar_ref[at, lanes] = reach[0]
            ai_ref[at, lanes] = reach[1]
            br_ref[at, lanes] = state[0]
            bi_ref[at, lanes] = state[1]
        for q, value in enumerate(reach + state):
            for k in range(ROWS):
                whole[q, k, pl.ds(i, 1), :] = value[k : k + 1]

    def close_segments():
        one_row, zero = jnp.ones((tiles, LANES), f32), jnp.zeros((tiles, LANES), f32)
        er, ei, sr, si = one_row, zero, zero, zero
        for k in range(ROWS):
            for q, value in enumerate((er, ei, sr, si)):
                pre[q, k] = value
            tr, ti, ur, ui = whole[0, k], whole[1, k], whole[2, k], whole[3, k]
            er, ei, sr, si = (
                tr * er - ti * ei,
                tr * ei + ti * er,
                tr * sr - ti * si + ur,
                tr * si + ti * sr + ui,
            )
        for q, value in enumerate((er, ei, sr, si)):
            ends[e, q] = value

    def ends_copy(i):
        return pltpu.make_async_remote_copy(
            ends.at[e], ends.at[e], ends_send.at[i], ends_recv.at[e], device_id={"ep": i, "tp": t}, device_id_type=MESH
        )

    def send_ends():
        close_segments()
        for i in range(1, n_ep):
            @pl.when(i > e)
            def _():
                ends_copy(i).start()

    def incoming():
        zero = jnp.zeros((tiles, LANES), f32)
        inc[0] = zero
        inc[1] = zero
        for i in range(n_ep - 1):
            @pl.when(i < e)
            def _():
                part = ends.at[i]
                pltpu.make_async_remote_copy(
                    part, part, ends_send.at[i], ends_recv.at[i], device_id={"ep": e, "tp": sib}, device_id_type=MESH
                ).wait_recv()
                tr, ti, ur, ui = ends[i, 0], ends[i, 1], ends[i, 2], ends[i, 3]
                sr, si = inc[0], inc[1]
                inc[0] = tr * sr - ti * si + ur
                inc[1] = tr * si + ti * sr + ui

    def split(value):
        high = value.astype(bf16)
        return high, (value - high.astype(f32)).astype(bf16)

    def read_tile(i):
        lanes = pl.ds(pl.multiple_of(i * LANES, LANES), LANES)
        ir, ii = inc[0, pl.ds(i, 1), :], inc[1, pl.ds(i, 1), :]
        pre_r, pre_i, pre_sr, pre_si = (pre[q, :, pl.ds(i, 1), :].reshape(ROWS, LANES) for q in range(4))
        enter_r = (pre_sr + pre_r * ir - pre_i * ii)[None]
        enter_i = (pre_si + pre_r * ii + pre_i * ir)[None]
        shape = (segment, ROWS, LANES)
        ar, ai = ar_ref[:, lanes].reshape(shape), ai_ref[:, lanes].reshape(shape)
        br, bi = br_ref[:, lanes].reshape(shape), bi_ref[:, lanes].reshape(shape)
        state_r = (br + ar * enter_r - ai * enter_i).reshape(positions, LANES)
        state_i = (bi + ar * enter_i + ai * enter_r).reshape(positions, LANES)
        wr, wi = wout[0, :, lanes], -wout[1, :, lanes]
        high_r, low_r = split(state_r)
        high_i, low_i = split(state_i)
        nt = ((1,), (1,))
        total[...] += (dot(high_r, wr, nt) + dot(low_r, wr, nt)) + (dot(high_i, wi, nt) + dot(low_i, wi, nt))

    def ssm_y_copy(yy):
        part = ssm.at[c, y]
        return pltpu.make_async_remote_copy(
            part, part, ssm_sem.at[0], ssm_sem.at[1], device_id={"ep": e, "tp": yy * 2 + c}, device_id_type=MESH
        )

    def ssm_sib_copy(yy):
        part = ssm.at[c, yy]
        return pltpu.make_async_remote_copy(
            part, part, ssm_sem.at[2], ssm_sem.at[3], device_id={"ep": e, "tp": sib}, device_id_type=MESH
        )

    def read_tiles(first, last):
        lax.fori_loop(first, last, lambda i, _: (read_tile(i), 0)[1], 0)

    def begin_read():
        incoming()
        total[...] = feed[...] * us[...].astype(f32)
        read_tiles(0, tiles // 2)

    def end_read():
        read_tiles(tiles // 2, tiles)
        value = total[...]
        inner = 0.7978845608028654 * (value + 0.044715 * (value * value * value))
        result = (0.5 * value * (1.0 + jnp.tanh(inner))).astype(bf16)
        unshuffle = ones_where(iota((positions, positions), 1) == (iota((positions, positions), 0) % segment) * ROWS + iota((positions, positions), 0) // segment)
        ssm[c, y] = dot(unshuffle, result).astype(bf16)
        for dy in range(1, n_y):
            ssm_y_copy(lax.rem(y + dy, n_y)).start()
        ssm_sib_copy(y).start()

    for k in range(14, 20):
        loads[k].wait()

    def tiles_between(first, last):
        lax.fori_loop(jnp.minimum(first, tiles), jnp.minimum(last, tiles), lambda i, _: (tile_work(i), 0)[1], 0)

    def arrive(s, piece):
        @pl.when((s >= 0) & (s < steps))
        def _():
            row, other = place(s)
            blk = block_of(row, other)
            token_copy(blk, piece, c, tok_sib.at[blk, piece], tok_recv.at[blk, piece], e, sib).wait_recv()

            @pl.when(other == 0)
            def _():
                forward(row, piece)

            sib_copy(blk, piece).start()

    def first_products(p, piece):
        def whole_rows(s):
            row, other = place(s)
            blk = block_of(row, other)
            token_copy(blk, piece, 1 - c, tok_sib.at[blk, piece], tok_recv_sib.at[blk, piece], e, sib).wait_recv()
            return tok[blk, piece_of(piece)]

        one_s, two_s = 2 * p - 1, 2 * p

        @pl.when(two_s < steps)
        def _():
            rows = jnp.concatenate([whole_rows(one_s), whole_rows(two_s)], axis=0)
            gated(rows, gate, up, [(one_s, piece_of(piece)), (two_s, piece_of(piece))])
            send_hidden(one_s, piece)
            send_hidden(two_s, piece)

        @pl.when((one_s < steps) & (two_s >= steps))
        def _():
            gated(whole_rows(one_s), gate, up, [(one_s, piece_of(piece))])
            send_hidden(one_s, piece)

    def held(s):
        return (s == 2) & (short < 1) & (steps >= 6)

    def last_product(s):
        row, other = place(s)
        blk = block_of(row, other)
        value = down_product(s, down).astype(bf16)

        @pl.when(blk == e)
        def _():
            ret[e] = value

        @pl.when(blk != e)
        def _():
            res[blk] = value

        @pl.when((blk != e) & jnp.logical_not(held(s)))
        def _():
            send_result(blk)


    def one(q, act):
        @pl.when((q >= 0) & (q < steps))
        def _():
            act(q)

    arrive(1, 0)
    arrive(2, 0)
    tiles_between(0, 1)

    def pair(p, carry):
        first_products(p, 0)

        @pl.when(p == 1)
        def _():
            tiles_between(1, 2)

        for piece in range(1, PIECES):
            arrive(2 * p - 1, piece)
            arrive(2 * p, piece)

        @pl.when((p == 3) & (short < 1) & (steps >= 6))
        def _():
            row, other = place(2)
            send_result(block_of(row, other))

        @pl.when(p == 1)
        def _():
            tiles_between(2, 3)

        @pl.when(p >= 2)
        def _():
            one(2 * p - 3, relay_hidden)

        for piece in range(1, PIECES):
            first_products(p, piece)

        @pl.when(p == 5)
        def _():
            end_read()

        @pl.when(p >= 2)
        def _():
            one(2 * p - 3, last_product)
            one(2 * p - 2, relay_hidden)

        arrive(2 * p + 1, 0)
        arrive(2 * p + 2, 0)

        @pl.when(p == 1)
        def _():
            relay_hidden(steps)
            relay_hidden(0)
            tiles_between(3, TILES_IN_FIRST)

        @pl.when(p == 2)
        def _():
            tiles_between(TILES_IN_FIRST, tiles)
            send_ends()

        @pl.when(p == 4)
        def _():
            begin_read()

        @pl.when(p >= 2)
        def _():
            one(2 * p - 2, last_product)

        return carry

    lax.fori_loop(1, steps // 2 + 2, pair, 0)
    last_product(0)
    shared_cols[...] = down_product(steps, sdown)

    span(ssm.at[c, pl.ds(0, n_y - 1)], ssm_sem.at[0], ssm_sem.at[1]).wait_recv()
    for dy in range(1, n_y):
        ssm_sib_copy(lax.rem(y + dy, n_y)).start()
    span(ssm.at[1 - c], ssm_sem.at[2], ssm_sem.at[3]).wait_recv()
    squares = jnp.zeros((positions, 1), f32)
    for cc in range(2):
        for yy in range(n_y):
            piece = ssm[cc, yy].astype(f32)
            squares = squares + jnp.sum(piece * piece, axis=-1, keepdims=True)
    factor = lax.rsqrt(squares / (channels * n_tp) + eps_norm)

    def gain_of(tt):
        if channels % LANES == 0:
            return mscale[:, tt * channels : (tt + 1) * channels]
        return mscale[tt : tt + 1, :]

    value = None
    for cc in range(2):
        for yy in range(n_y):
            tt = yy * 2 + cc
            normed = (ssm[cc, yy].astype(f32) * factor * gain_of(tt)).astype(bf16)
            term = dot(normed, mweight[tt * channels : (tt + 1) * channels, :])
            value = term if value is None else value + term
    mixed_ref[...] = value.astype(bf16)
    mixed_store = pltpu.make_async_copy(mixed_ref, mixed_hbm, store_sem.at[0])
    mixed_store.start()

    taken = jnp.zeros((n_ep, token_rows), f32)
    for k in range(routes.shape[0]):
        taken = taken + jnp.where(iota((n_ep, token_rows), 0) == routes[k : k + 1, :], chosen[k : k + 1, :], 0.0)
    shares[...] = taken.T

    def share_of(i):
        return jnp.sum(jnp.where(iota((token_rows, n_ep), 1) == i, shares[...], 0.0), axis=1, keepdims=True)

    late_weight[...] = jnp.broadcast_to(share_of(late_source), late_weight.shape)
    weight_store = pltpu.make_async_copy(late_weight, weight_hbm, store_sem.at[2])
    weight_store.start()

    def combine(s, carry):
        row, other = place(s)
        i = block_of(row, other)

        @pl.when((i != e) & (i != late_source))
        def _():
            from_expert(i, ret.at[i]).wait_recv()

        @pl.when(i != late_source)
        def _():
            shared_cols[...] += ret[i].astype(f32) * share_of(i)

        return carry

    lax.fori_loop(0, steps, combine, 0)
    sum_store = pltpu.make_async_copy(shared_cols, sum_hbm, store_sem.at[1])
    sum_store.start()

    def drain(s, carry):
        @pl.when(s != e)
        def _():
            for piece in range(PIECES):
                sib_copy(s, piece).wait_send()
            res_copy(s, ret.at[e]).wait_send()

        @pl.when(s > e)
        def _():
            ends_copy(s).wait_send()

        return carry

    lax.fori_loop(0, n_ep, drain, 0)

    def drain_line(row, carry):
        for piece in range(PIECES):
            @pl.when((row <= a) & (a + 1 < n_line))
            def _():
                up_copy(row, piece).wait_send()

            @pl.when((row >= a) & (a >= 1))
            def _():
                dn_copy(row, piece).wait_send()

            x_copy(row, piece).wait_send()
        return carry

    lax.fori_loop(0, n_line, drain_line, 0)

    def drain_hidden(s, carry):
        for piece in range(PIECES):
            from_y(s, piece).wait_send()
            from_sib(s, piece, c).wait_send()
        return carry

    lax.fori_loop(0, steps + 1, drain_hidden, 0)
    span(ssm.at[c, pl.ds(0, n_y - 1)], ssm_sem.at[0], ssm_sem.at[1]).wait_send()
    span(ssm.at[c], ssm_sem.at[2], ssm_sem.at[3]).wait_send()
    mixed_store.wait()
    weight_store.wait()
    sum_store.wait()
    from_expert(late_source, late_hbm).wait_recv()


def hand_over(mixed, sums, late, weight):
    def finish(mixed_in, sum_in, late_in, weight_in, mixed_ref, moe_ref):
        mixed_ref[...] = mixed_in[...]
        moe_ref[...] = (sum_in[...] + late_in[...].astype(f32) * weight_in[:, 0:1]).astype(bf16)

    def whole(v):
        return pl.BlockSpec(v.shape, lambda i: (0, 0))

    return pl.pallas_call(
        finish,
        grid=(1,),
        in_specs=[whole(v) for v in (mixed, sums, late, weight)],
        out_specs=[whole(mixed), whole(late)],
        out_shape=[jax.ShapeDtypeStruct(v.shape, v.dtype) for v in (mixed, late)],
        name="hand_over",
    )(mixed, sums, late, weight)


def on_device(*operands):
    (
        u, logs, losses, eigen, frequency, group_in, group_out, feed, mixer_scale, mixer_weight,
        x, gain, routes, chosen, gate, up, down, shared_gate, shared_up, shared_down,
    ) = operands
    n_ep, n_tp = lax.axis_size("ep"), lax.axis_size("tp")
    positions, channels = u.shape
    groups, states = eigen.shape
    lanes_all = groups * states
    tiles = lanes_all // LANES
    token_rows, width = x.shape
    hidden, columns = gate.shape[2], down.shape[2]
    group_in = group_in.transpose(0, 1, 3, 2).reshape(2, channels, states)
    group_out = group_out.reshape(2, channels, states)
    feed = feed.reshape(1, channels)
    mixer_scale = mixer_scale.reshape((1, -1) if channels % LANES == 0 else (n_tp, channels))
    gain = gain.reshape(1, width)
    routes, chosen = routes.T, chosen.T
    given = (
        u, logs, losses, eigen, frequency, group_in, group_out, feed, mixer_scale, mixer_weight,
        x, gain, routes, chosen, gate, up, down, shared_gate, shared_up, shared_down,
    )
    local = [
        pltpu.VMEM(g.shape[1:] if k in (14, 15, 16) else g.shape, g.dtype) for k, g in enumerate(given)
    ]
    slot = -(-groups // 16) * 16
    wide = pltpu.VMEM((positions, lanes_all), f32)
    dma = pltpu.SemaphoreType.DMA
    scratch = local + [
        pltpu.VMEM((n_ep, token_rows, width), bf16),
        pltpu.VMEM((n_ep + 1, 2, n_tp // 2, token_rows, hidden), bf16),
        pltpu.VMEM((n_ep, token_rows, columns), bf16),
        pltpu.VMEM((n_ep, token_rows, columns), bf16),
        pltpu.VMEM((n_ep, 4, tiles, LANES), f32),
        pltpu.VMEM((2, n_tp // 2, positions, channels), bf16),
        pltpu.VMEM((positions, channels), bf16),
        pltpu.VMEM((2, 3 * slot, positions), bf16),
        pltpu.VMEM((tiles, LANES), f32),
        pltpu.VMEM((tiles, LANES), f32),
        pltpu.VMEM((2, channels, lanes_all), bf16),
        pltpu.VMEM((2, channels, lanes_all), bf16),
        wide, wide, wide, wide,
        pltpu.VMEM((4, ROWS, tiles, LANES), f32),
        pltpu.VMEM((4, ROWS, tiles, LANES), f32),
        pltpu.VMEM((2, tiles, LANES), f32),
        pltpu.VMEM((positions, channels), f32),
        pltpu.VMEM((token_rows, columns), f32),
        pltpu.VMEM((token_rows, n_ep), f32),
        dma((len(given),)),
        dma((n_ep // 2, PIECES)), dma((n_ep // 2, PIECES)), dma((n_ep // 2, PIECES)),
        dma((n_ep, PIECES)), dma((n_ep, PIECES)), dma((n_ep, PIECES)),
        dma((n_ep + 1, PIECES)), dma((n_ep + 1, PIECES)), dma((n_ep + 1, PIECES)), dma((n_ep + 1, PIECES)),
        dma((n_ep,)), dma((n_ep,)), dma((n_ep,)), dma((n_ep,)),
        dma((4,)),
        dma((3,)),
        pltpu.VMEM((positions, columns), bf16),
        pltpu.VMEM((token_rows, LANES), f32),
    ]
    parts_out = pl.pallas_call(
        functools.partial(body, n_ep, n_tp),
        out_shape=[
            jax.ShapeDtypeStruct((positions, columns), bf16),
            jax.ShapeDtypeStruct((token_rows, columns), f32),
            jax.ShapeDtypeStruct((token_rows, columns), bf16),
            jax.ShapeDtypeStruct((token_rows, LANES), f32),
        ],
        in_specs=[pl.BlockSpec(memory_space=pl.ANY)] * len(given),
        out_specs=[pl.BlockSpec(memory_space=pl.ANY)] * 4,
        scratch_shapes=scratch,
        compiler_params=pltpu.CompilerParams(
            collective_id=0, has_side_effects=True, vmem_limit_bytes=VMEM_BYTES
        ),
        name="both_batches",
    )(*given)
    return hand_over(*parts_out)


def solution(mesh):
    return jax.shard_map(
        on_device,
        mesh=mesh,
        in_specs=(
            P("ep", "tp"),
            P("tp", "ep"),
            P("tp", "ep"),
            P("tp", None),
            P("tp", None),
            P(None, "tp", None, None),
            P(None, "tp", None, None),
            P("tp"),
            P(),
            P(None, "tp"),
            P("ep", None),
            P(),
            P("ep", None),
            P("ep", None),
            P("ep", None, "tp"),
            P("ep", None, "tp"),
            P("ep", None, "tp"),
            P(None, "tp"),
            P(None, "tp"),
            P(None, "tp"),
        ),
        out_specs=(P("ep", "tp"), P("ep", "tp")),
        check_vma=False,
    )
```

```python
import functools

import jax
import jax.numpy as jnp
from jax import lax
from jax.experimental import pallas as pl
from jax.experimental.pallas import tpu as pltpu
from jax.sharding import PartitionSpec as P

eps_norm = 1e-06
LANES = 128
ROWS = 8
MESH = pl.DeviceIdType.MESH
bf16, f32 = jnp.bfloat16, jnp.float32
PIECES = 2
TILES_IN_FIRST = 6
VMEM_BYTES = 62 * 1024 * 1024


def cos_sin(angle):
    turns = jnp.floor(angle * 0.6366197723675814 + 0.5)
    rest = ((angle - turns * 1.5703125) - turns * 4.837512969970703125e-4) - turns * 7.549789954891882e-8
    square = rest * rest
    sine = rest + rest * square * (
        -1.6666654611e-1 + square * (8.3321608736e-3 + square * -1.9515295891e-4)
    )
    cosine = (
        1.0
        - 0.5 * square
        + square
        * square
        * (
            4.166664568298827e-2
            + square * (-1.388731625493765e-3 + square * 2.443315711809948e-5)
        )
    )
    quarter = turns.astype(jnp.int32)
    odd = (quarter & 1) == 1
    out_cos = jnp.where(odd, sine, cosine)
    out_sin = jnp.where(odd, cosine, sine)
    out_cos = jnp.where(((quarter + 1) & 2) == 2, -out_cos, out_cos)
    out_sin = jnp.where((quarter & 2) == 2, -out_sin, out_sin)
    return out_cos, out_sin


def one_minus_exp_neg(y):
    series = y * (
        1.0
        - y * (1.0 / 2)
        * (1.0 - y * (1.0 / 3) * (1.0 - y * (1.0 / 4) * (1.0 - y * (1.0 / 5) * (1.0 - y * (1.0 / 6)))))
    )
    return jnp.where(y < 0.3, series, 1.0 - jnp.exp(-y))


def dot(a, b, dims=((1,), (0,)), precision=None):
    return lax.dot_general(a, b, (dims, ((), ())), preferred_element_type=f32, precision=precision)


def iota(shape, axis):
    return lax.broadcasted_iota(jnp.int32, shape, axis)


def ones_where(condition, dtype=bf16):
    return jnp.where(condition, 1.0, 0.0).astype(dtype)


def scaled_rows(values, gain):
    widened = values.astype(f32)
    factor = lax.rsqrt(jnp.mean(widened * widened, axis=-1, keepdims=True) + eps_norm)
    return (widened * factor * gain).astype(bf16)


def body(
    n_ep, n_tp,
    u_hbm, logs_hbm, loss_hbm, eig_hbm, freq_hbm, gin_hbm, gout_hbm, feed_hbm, mscale_hbm, mweight_hbm,
    x_hbm, gain_hbm, routes_hbm, chosen_hbm, gate_hbm, up_hbm, down_hbm, sgate_hbm, sup_hbm, sdown_hbm,
    mixed_hbm, sum_hbm, late_hbm, weight_hbm,
    u, logs, loss, eig, freq, gin, gout, feed, mscale, mweight,
    x, gain, routes, chosen, gate, up, down, sgate, sup, sdown,
    tok, hid, res, ret, ends, ssm,
    us, parts, eigrow, freqrow, win, wout, ar_ref, ai_ref, br_ref, bi_ref, whole, pre, inc, total, shared_cols, shares,
    load_sem,
    tok_up, tok_dn, tok_x, tok_sib, tok_recv, tok_recv_sib,
    hid_send_y, hid_send_sib, hid_recv_y, hid_recv_sib,
    res_send, res_recv, ends_sem,
    ssm_sem, store_sem, mixed_ref, late_weight,
):
    e, t = lax.axis_index("ep"), lax.axis_index("tp")
    n_line, n_y = n_ep // 2, n_tp // 2
    a, b = e // 2, e % 2
    y, c = t // 2, t % 2
    steps = n_ep
    token_rows, width = x.shape
    half = width // 2
    hidden = gate.shape[1]
    columns = down.shape[1]
    positions, channels = u.shape
    groups, states = eig.shape
    group_ch = channels // groups
    lanes_all = groups * states
    tiles = lanes_all // LANES
    per_tile = LANES // states
    segment = positions // ROWS

    barrier = pltpu.get_barrier_semaphore()
    for i in range(n_ep):
        @pl.when(e != i)
        def _():
            pl.semaphore_signal(barrier, inc=1, device_id={"ep": i, "tp": t}, device_id_type=MESH)
    for i in range(n_tp):
        @pl.when(t != i)
        def _():
            pl.semaphore_signal(barrier, inc=1, device_id={"ep": e, "tp": i}, device_id_type=MESH)

    pairs = [
        (x_hbm, x), (gain_hbm, gain), (sgate_hbm, sgate), (sup_hbm, sup), (gate_hbm.at[0], gate), (up_hbm.at[0], up),
        (u_hbm, u), (logs_hbm, logs), (loss_hbm, loss), (eig_hbm, eig), (freq_hbm, freq), (gin_hbm, gin),
        (gout_hbm, gout), (feed_hbm, feed), (down_hbm.at[0], down), (sdown_hbm, sdown), (mscale_hbm, mscale),
        (mweight_hbm, mweight), (routes_hbm, routes), (chosen_hbm, chosen),
    ]
    loads = [pltpu.make_async_copy(src, dst, load_sem.at[k]) for k, (src, dst) in enumerate(pairs)]
    for load in loads:
        load.start()

    left, right = a, n_line - 1 - a
    short = jnp.minimum(left, right)
    sign_long = jnp.where(left <= right, 1, -1)

    def near(k):
        odd = k % 2
        alternating = jnp.where(odd == 1, sign_long, -sign_long) * ((k + 1) // 2)
        beyond = sign_long * (k - short)
        return a + jnp.where(k <= 2 * short, alternating, beyond)

    def place(s):
        last = s == steps - 1
        odd = s % 2 == 1
        k = jnp.where(last, n_line - 1, jnp.where(odd, (s + 1) // 2, s // 2 - 1))
        other = jnp.where(last, 1, jnp.where(odd, 0, 1))
        own_first = short >= 1
        swapped = jnp.where(s == n_line, 1, jnp.where(s == n_line + 1, 0, s - n_line))
        k = jnp.where(own_first, jnp.where(s < n_line, s, swapped), k)
        other = jnp.where(own_first, jnp.where(s < n_line, 0, 1), other)
        k = jnp.where(s == 0, 0, k)
        other = jnp.where(s == 0, 0, other)
        row = jnp.where(k == 0, a, near(k))
        return row, other

    def block_of(row, other):
        return row * 2 + jnp.where(other == 1, 1 - b, b)

    piece_rows = token_rows // PIECES

    def token_copy(blk, piece, half_index, send, recv, ep, tp):
        rows = pl.ds(pl.multiple_of(piece * piece_rows, piece_rows), piece_rows)
        part = tok.at[blk, rows, pl.ds(pl.multiple_of(half_index * half, half), half)]
        return pltpu.make_async_remote_copy(
            part, part, send, recv, device_id={"ep": ep, "tp": tp}, device_id_type=MESH
        )

    sib = y * 2 + 1 - c

    def line_copy(row, piece, sent, ep):
        blk = row * 2 + b
        return token_copy(blk, piece, c, sent, tok_recv.at[blk, piece], ep, t)

    def up_copy(row, piece):
        return line_copy(row, piece, tok_up.at[row, piece], jnp.minimum(e + 2, n_ep - 2 + b))

    def dn_copy(row, piece):
        return line_copy(row, piece, tok_dn.at[row, piece], jnp.maximum(e - 2, b))

    def x_copy(row, piece):
        return line_copy(row, piece, tok_x.at[0], a * 2 + 1 - b)

    def sib_copy(blk, piece):
        return token_copy(blk, piece, c, tok_sib.at[0], tok_recv_sib.at[blk, piece], e, sib)

    def forward(row, piece):
        @pl.when((row <= a) & (a + 1 < n_line))
        def _():
            up_copy(row, piece).start()

        @pl.when((row >= a) & (a >= 1))
        def _():
            dn_copy(row, piece).start()

    def piece_of(piece):
        return pl.ds(piece * piece_rows, piece_rows)

    def hid_y_copy(s, piece, yy):
        part = hid.at[s, c, y, piece_of(piece)]
        return pltpu.make_async_remote_copy(
            part, part, hid_send_y.at[0], hid_recv_y.at[s],
            device_id={"ep": e, "tp": yy * 2 + c}, device_id_type=MESH,
        )

    def hid_sib_copy(s, piece, yy):
        part = hid.at[s, c, yy, piece_of(piece)]
        return pltpu.make_async_remote_copy(
            part, part, hid_send_sib.at[0], hid_recv_sib.at[s],
            device_id={"ep": e, "tp": sib}, device_id_type=MESH,
        )

    def span(ref, send, recv):
        return pltpu.make_async_remote_copy(
            ref, ref, send, recv, device_id={"ep": e, "tp": sib}, device_id_type=MESH
        )

    def from_y(s):
        return span(hid.at[s, c, pl.ds(0, n_y - 1)], hid_send_y.at[0], hid_recv_y.at[s])

    def from_sib(s):
        return span(hid.at[s, 1 - c], hid_send_sib.at[0], hid_recv_sib.at[s])

    def gated(rows, gate_w, up_w, targets):
        block = min(256, hidden)
        for n in range(hidden // block):
            cols = pl.ds(n * block, block)
            gate_part = dot(rows, gate_w[:, cols])
            up_part = dot(rows, up_w[:, cols])
            value = (gate_part / (1.0 + jnp.exp(-gate_part)) * up_part).astype(bf16)
            done = 0
            for s, into in targets:
                hid[s, c, y, into, cols] = value[done : done + into.size]
                done += into.size

    def send_hidden(s, piece):
        for dy in range(1, n_y):
            hid_y_copy(s, piece, lax.rem(y + dy, n_y)).start()
        hid_sib_copy(s, piece, y).start()

    def relay_hidden(s):
        from_y(s).wait_recv()
        for dy in range(1, n_y):
            part = hid.at[s, c, lax.rem(y + dy, n_y)]
            span(part, hid_send_sib.at[0], hid_recv_sib.at[s]).start()

    def down_product(s, weight):
        from_sib(s).wait_recv()
        value = None
        for cc in range(2):
            for yy in range(n_y):
                rows = (yy * 2 + cc) * hidden
                term = dot(hid[s, cc, yy], weight[rows : rows + hidden, :])
                value = term if value is None else value + term
        return value

    late_target = lax.rem(a + n_line // 2, n_line) * 2 + 1 - b
    late_source = lax.rem(a + n_line - n_line // 2, n_line) * 2 + 1 - b

    def res_copy(blk, into):
        return pltpu.make_async_remote_copy(
            res.at[blk], into, res_send.at[0], res_recv.at[e], device_id={"ep": blk, "tp": t}, device_id_type=MESH
        )

    def send_result(blk):
        @pl.when(blk == late_target)
        def _():
            res_copy(blk, late_hbm).start()

        @pl.when(blk != late_target)
        def _():
            res_copy(blk, ret.at[e]).start()

    def from_expert(i, into):
        return pltpu.make_async_remote_copy(
            into, into, res_send.at[0], res_recv.at[i], device_id={"ep": e, "tp": sib}, device_id_type=MESH
        )

    loads[0].wait()
    loads[1].wait()
    tok[e] = scaled_rows(x[...], gain[...])
    pl.semaphore_wait(barrier, n_ep + n_tp - 2)
    for piece in range(PIECES):
        forward(a, piece)
        x_copy(a, piece).start()

    loads[2].wait()
    loads[3].wait()
    everything = pl.ds(0, token_rows)
    gated(tok[e], sgate, sup, [(steps, everything)])
    for piece in range(PIECES):
        send_hidden(steps, piece)
    loads[4].wait()
    loads[5].wait()
    gated(tok[e], gate, up, [(0, everything)])
    for piece in range(PIECES):
        send_hidden(0, piece)

    for k in range(6, 14):
        loads[k].wait()
    shuffle = ones_where(iota((positions, positions), 1) == (iota((positions, positions), 0) % ROWS) * segment + iota((positions, positions), 0) // ROWS)
    us[...] = dot(shuffle, u[...]).astype(bf16)
    parts[...] = jnp.zeros(parts.shape, bf16)
    slot = parts.shape[1] // 3
    for q, table in enumerate((jnp.exp(logs[...]), loss[...])):
        rest = table
        for r in range(3):
            piece = rest.astype(bf16)
            rest = rest - piece.astype(f32)
            parts[q, r * slot : r * slot + groups, :] = dot(piece, shuffle, ((1,), (1,))).astype(bf16)
    spread = ones_where(iota((states, LANES), 1) % states == iota((states, LANES), 0), f32)
    for table, rows_ref in ((eig, eigrow), (freq, freqrow)):
        wide = dot(table[...], spread, precision=lax.Precision.HIGHEST)
        row = jnp.zeros((tiles, LANES), f32)
        for h in range(per_tile):
            pick = ones_where(iota((tiles, groups), 1) == iota((tiles, groups), 0) * per_tile + h, f32)
            picked = dot(pick, wide, precision=lax.Precision.HIGHEST)
            row = jnp.where(iota((tiles, LANES), 1) // states == h, picked, row)
        rows_ref[...] = row
    spread_all = ones_where(iota((states, lanes_all), 1) % states == iota((states, lanes_all), 0))
    own_group = iota((channels, lanes_all), 0) // group_ch == iota((channels, lanes_all), 1) // states
    for r in range(2):
        win[r] = jnp.where(own_group, dot(gin[r], spread_all), 0.0).astype(bf16)
        wout[r] = jnp.where(own_group, dot(gout[r], spread_all), 0.0).astype(bf16)

    def tile_work(i):
        lanes = pl.ds(pl.multiple_of(i * LANES, LANES), LANES)
        slot_rows = 3 * slot
        own = iota((slot_rows, LANES), 0) % slot == per_tile * i + iota((slot_rows, LANES), 1) // states
        select = ones_where(own)
        step_wide = dot(parts[0], select, ((0,), (0,)))
        loss_wide = dot(parts[1], select, ((0,), (0,)))
        loss_rate = eigrow[pl.ds(i, 1), :] * step_wide
        magnitude = jnp.exp(loss_wide - loss_rate)
        cosine, sine = cos_sin(freqrow[pl.ds(i, 1), :] * step_wide)
        scaling = jnp.sqrt(one_minus_exp_neg(2.0 * loss_rate))
        ar_ref[:, lanes] = magnitude * cosine
        ai_ref[:, lanes] = magnitude * sine
        br_ref[:, lanes] = scaling * dot(us[...], win[0, :, lanes])
        bi_ref[:, lanes] = scaling * dot(us[...], win[1, :, lanes])
        reach = jnp.ones((ROWS, LANES), f32), jnp.zeros((ROWS, LANES), f32)
        state = jnp.zeros((ROWS, LANES), f32), jnp.zeros((ROWS, LANES), f32)
        for j in range(segment):
            at = pl.ds(j * ROWS, ROWS)
            ar, ai, br, bi = ar_ref[at, lanes], ai_ref[at, lanes], br_ref[at, lanes], bi_ref[at, lanes]
            reach = ar * reach[0] - ai * reach[1], ar * reach[1] + ai * reach[0]
            state = ar * state[0] - ai * state[1] + br, ar * state[1] + ai * state[0] + bi
            ar_ref[at, lanes] = reach[0]
            ai_ref[at, lanes] = reach[1]
            br_ref[at, lanes] = state[0]
            bi_ref[at, lanes] = state[1]
        for q, value in enumerate(reach + state):
            for k in range(ROWS):
                whole[q, k, pl.ds(i, 1), :] = value[k : k + 1]

    def close_segments():
        one_row, zero = jnp.ones((tiles, LANES), f32), jnp.zeros((tiles, LANES), f32)
        er, ei, sr, si = one_row, zero, zero, zero
        for k in range(ROWS):
            for q, value in enumerate((er, ei, sr, si)):
                pre[q, k] = value
            tr, ti, ur, ui = whole[0, k], whole[1, k], whole[2, k], whole[3, k]
            er, ei, sr, si = (
                tr * er - ti * ei,
                tr * ei + ti * er,
                tr * sr - ti * si + ur,
                tr * si + ti * sr + ui,
            )
        for q, value in enumerate((er, ei, sr, si)):
            ends[e, q] = value

    def ends_copy(i):
        return pltpu.make_async_remote_copy(
            ends.at[e], ends.at[e], ends_sem.at[0], ends_sem.at[1], device_id={"ep": i, "tp": t}, device_id_type=MESH
        )

    def send_ends():
        close_segments()
        for i in range(n_ep):
            @pl.when(i != e)
            def _():
                ends_copy(i).start()

    def all_ends():
        return span(ends.at[pl.ds(0, n_ep - 1)], ends_sem.at[0], ends_sem.at[1])

    def incoming():
        zero = jnp.zeros((tiles, LANES), f32)
        inc[0] = zero
        inc[1] = zero
        all_ends().wait_recv()
        for i in range(n_ep - 1):
            @pl.when(i < e)
            def _():
                tr, ti, ur, ui = ends[i, 0], ends[i, 1], ends[i, 2], ends[i, 3]
                sr, si = inc[0], inc[1]
                inc[0] = tr * sr - ti * si + ur
                inc[1] = tr * si + ti * sr + ui

    def split(value):
        high = value.astype(bf16)
        return high, (value - high.astype(f32)).astype(bf16)

    def read_tile(i):
        lanes = pl.ds(pl.multiple_of(i * LANES, LANES), LANES)
        ir, ii = inc[0, pl.ds(i, 1), :], inc[1, pl.ds(i, 1), :]
        pre_r, pre_i, pre_sr, pre_si = (pre[q, :, pl.ds(i, 1), :].reshape(ROWS, LANES) for q in range(4))
        enter_r = (pre_sr + pre_r * ir - pre_i * ii)[None]
        enter_i = (pre_si + pre_r * ii + pre_i * ir)[None]
        shape = (segment, ROWS, LANES)
        ar, ai = ar_ref[:, lanes].reshape(shape), ai_ref[:, lanes].reshape(shape)
        br, bi = br_ref[:, lanes].reshape(shape), bi_ref[:, lanes].reshape(shape)
        state_r = (br + ar * enter_r - ai * enter_i).reshape(positions, LANES)
        state_i = (bi + ar * enter_i + ai * enter_r).reshape(positions, LANES)
        wr, wi = wout[0, :, lanes], -wout[1, :, lanes]
        high_r, low_r = split(state_r)
        high_i, low_i = split(state_i)
        nt = ((1,), (1,))
        total[...] += (dot(high_r, wr, nt) + dot(low_r, wr, nt)) + (dot(high_i, wi, nt) + dot(low_i, wi, nt))

    def ssm_y_copy(yy):
        part = ssm.at[c, y]
        return pltpu.make_async_remote_copy(
            part, part, ssm_sem.at[0], ssm_sem.at[1], device_id={"ep": e, "tp": yy * 2 + c}, device_id_type=MESH
        )

    def ssm_sib_copy(yy):
        part = ssm.at[c, yy]
        return pltpu.make_async_remote_copy(
            part, part, ssm_sem.at[2], ssm_sem.at[3], device_id={"ep": e, "tp": sib}, device_id_type=MESH
        )

    def read_tiles(first, last):
        lax.fori_loop(first, last, lambda i, _: (read_tile(i), 0)[1], 0)

    def begin_read():
        incoming()
        total[...] = feed[...] * us[...].astype(f32)
        read_tiles(0, tiles // 2)

    def end_read():
        read_tiles(tiles // 2, tiles)
        value = total[...]
        inner = 0.7978845608028654 * (value + 0.044715 * (value * value * value))
        result = (0.5 * value * (1.0 + jnp.tanh(inner))).astype(bf16)
        unshuffle = ones_where(iota((positions, positions), 1) == (iota((positions, positions), 0) % segment) * ROWS + iota((positions, positions), 0) // segment)
        ssm[c, y] = dot(unshuffle, result).astype(bf16)
        for dy in range(1, n_y):
            ssm_y_copy(lax.rem(y + dy, n_y)).start()
        ssm_sib_copy(y).start()

    for k in range(14, 20):
        loads[k].wait()

    def tiles_between(first, last):
        lax.fori_loop(jnp.minimum(first, tiles), jnp.minimum(last, tiles), lambda i, _: (tile_work(i), 0)[1], 0)

    def arrive(s, piece):
        @pl.when((s >= 0) & (s < steps))
        def _():
            row, other = place(s)
            blk = block_of(row, other)
            token_copy(blk, piece, c, tok_sib.at[0], tok_recv.at[blk, piece], e, sib).wait_recv()

            later = (s == 2) & (short >= 1)

            @pl.when(other == 0)
            def _():
                forward(row, piece)

            if piece == PIECES - 1:
                @pl.when((other == 0) & later)
                def _():
                    for early in range(PIECES - 1):
                        x_copy(row, early).start()

            @pl.when((other == 0) & (jnp.logical_not(later) | (piece == PIECES - 1)))
            def _():
                x_copy(row, piece).start()

            sib_copy(blk, piece).start()

    def first_products(p, piece):
        def whole_rows(s):
            row, other = place(s)
            blk = block_of(row, other)
            token_copy(blk, piece, 1 - c, tok_sib.at[0], tok_recv_sib.at[blk, piece], e, sib).wait_recv()
            return tok[blk, piece_of(piece)]

        one_s, two_s = 2 * p - 1, 2 * p

        @pl.when(two_s < steps)
        def _():
            rows = jnp.concatenate([whole_rows(one_s), whole_rows(two_s)], axis=0)
            gated(rows, gate, up, [(one_s, piece_of(piece)), (two_s, piece_of(piece))])
            send_hidden(one_s, piece)
            send_hidden(two_s, piece)

        @pl.when((one_s < steps) & (two_s >= steps))
        def _():
            gated(whole_rows(one_s), gate, up, [(one_s, piece_of(piece))])
            send_hidden(one_s, piece)

    def held(s):
        return (s == 2) & (short < 1) & (steps >= 6)

    def last_product(s):
        row, other = place(s)
        blk = block_of(row, other)
        value = down_product(s, down).astype(bf16)

        @pl.when(blk == e)
        def _():
            ret[e] = value

        @pl.when(blk != e)
        def _():
            res[blk] = value

        @pl.when((blk != e) & jnp.logical_not(held(s)))
        def _():
            send_result(blk)


    def one(q, act):
        @pl.when((q >= 0) & (q < steps))
        def _():
            act(q)

    arrive(1, 0)
    arrive(2, 0)
    tiles_between(0, 1)

    def pair(p, carry):
        first_products(p, 0)

        @pl.when(p == 1)
        def _():
            tiles_between(1, 2)

        @pl.when(p == 3)
        def _():
            one(2 * p - 3, relay_hidden)

        for piece in range(1, PIECES):
            arrive(2 * p - 1, piece)
            arrive(2 * p, piece)

        @pl.when((p == 3) & (short < 1) & (steps >= 6))
        def _():
            row, other = place(2)
            send_result(block_of(row, other))

        @pl.when(p == 1)
        def _():
            tiles_between(2, 3)

        @pl.when(p == 2)
        def _():
            one(2 * p - 3, relay_hidden)

        @pl.when(p == 3)
        def _():
            one(2 * p - 3, last_product)

        for piece in range(1, PIECES):
            first_products(p, piece)

        @pl.when(p >= 4)
        def _():
            one(2 * p - 3, relay_hidden)

        @pl.when(p == 5)
        def _():
            end_read()

        @pl.when(p >= 4)
        def _():
            one(2 * p - 2, relay_hidden)
            one(2 * p - 3, last_product)

        @pl.when(p == 2)
        def _():
            one(2 * p - 3, last_product)

        @pl.when((p == 2) | (p == 3))
        def _():
            one(2 * p - 2, relay_hidden)

        arrive(2 * p + 1, 0)
        arrive(2 * p + 2, 0)

        @pl.when(p == 1)
        def _():
            relay_hidden(steps)
            relay_hidden(0)
            tiles_between(3, TILES_IN_FIRST)

        @pl.when(p == 2)
        def _():
            tiles_between(TILES_IN_FIRST, tiles)
            send_ends()

        @pl.when(p == 4)
        def _():
            begin_read()

        @pl.when(p >= 2)
        def _():
            one(2 * p - 2, last_product)

        return carry

    lax.fori_loop(1, steps // 2 + 2, pair, 0)
    last_product(0)
    shared_cols[...] = down_product(steps, sdown)

    span(ssm.at[c, pl.ds(0, n_y - 1)], ssm_sem.at[0], ssm_sem.at[1]).wait_recv()
    for dy in range(1, n_y):
        ssm_sib_copy(lax.rem(y + dy, n_y)).start()
    span(ssm.at[1 - c], ssm_sem.at[2], ssm_sem.at[3]).wait_recv()
    squares = jnp.zeros((positions, 1), f32)
    for cc in range(2):
        for yy in range(n_y):
            piece = ssm[cc, yy].astype(f32)
            squares = squares + jnp.sum(piece * piece, axis=-1, keepdims=True)
    factor = lax.rsqrt(squares / (channels * n_tp) + eps_norm)

    def gain_of(tt):
        if channels % LANES == 0:
            return mscale[:, tt * channels : (tt + 1) * channels]
        return mscale[tt : tt + 1, :]

    value = None
    for cc in range(2):
        for yy in range(n_y):
            tt = yy * 2 + cc
            normed = (ssm[cc, yy].astype(f32) * factor * gain_of(tt)).astype(bf16)
            term = dot(normed, mweight[tt * channels : (tt + 1) * channels, :])
            value = term if value is None else value + term
    mixed_ref[...] = value.astype(bf16)
    mixed_store = pltpu.make_async_copy(mixed_ref, mixed_hbm, store_sem.at[0])
    mixed_store.start()

    taken = jnp.zeros((n_ep, token_rows), f32)
    for k in range(routes.shape[0]):
        taken = taken + jnp.where(iota((n_ep, token_rows), 0) == routes[k : k + 1, :], chosen[k : k + 1, :], 0.0)
    shares[...] = taken.T

    def share_of(i):
        return jnp.sum(jnp.where(iota((token_rows, n_ep), 1) == i, shares[...], 0.0), axis=1, keepdims=True)

    late_weight[...] = jnp.broadcast_to(share_of(late_source), late_weight.shape)
    weight_store = pltpu.make_async_copy(late_weight, weight_hbm, store_sem.at[2])
    weight_store.start()

    def combine(s, carry):
        row, other = place(s)
        i = block_of(row, other)

        @pl.when((i != e) & (i != late_source))
        def _():
            from_expert(i, ret.at[i]).wait_recv()

        @pl.when(i != late_source)
        def _():
            shared_cols[...] += ret[i].astype(f32) * share_of(i)

        return carry

    lax.fori_loop(0, steps, combine, 0)
    sum_store = pltpu.make_async_copy(shared_cols, sum_hbm, store_sem.at[1])
    sum_store.start()

    own_half = pl.ds(pl.multiple_of(c * half, half), half)
    span(tok.at[pl.ds(0, n_ep - 1), :, own_half], tok_sib.at[0], tok_recv.at[0, 0]).wait_send()
    span(tok.at[pl.ds(0, n_line), :, own_half], tok_x.at[0], tok_recv.at[0, 0]).wait_send()
    span(res.at[pl.ds(0, n_ep - 1)], res_send.at[0], res_recv.at[0]).wait_send()
    all_ends().wait_send()

    def drain_line(row, carry):
        for piece in range(PIECES):
            @pl.when((row <= a) & (a + 1 < n_line))
            def _():
                up_copy(row, piece).wait_send()

            @pl.when((row >= a) & (a >= 1))
            def _():
                dn_copy(row, piece).wait_send()

        return carry

    lax.fori_loop(0, n_line, drain_line, 0)

    span(hid.at[:, c, pl.ds(0, n_y - 1)], hid_send_y.at[0], hid_recv_y.at[0]).wait_send()
    span(hid.at[:, c], hid_send_sib.at[0], hid_recv_sib.at[0]).wait_send()
    span(ssm.at[c, pl.ds(0, n_y - 1)], ssm_sem.at[0], ssm_sem.at[1]).wait_send()
    span(ssm.at[c], ssm_sem.at[2], ssm_sem.at[3]).wait_send()
    mixed_store.wait()
    weight_store.wait()
    sum_store.wait()
    from_expert(late_source, late_hbm).wait_recv()


def hand_over(mixed, sums, late, weight):
    def finish(mixed_in, sum_in, late_in, weight_in, mixed_ref, moe_ref):
        mixed_ref[...] = mixed_in[...]
        moe_ref[...] = (sum_in[...] + late_in[...].astype(f32) * weight_in[:, 0:1]).astype(bf16)

    def whole(v):
        return pl.BlockSpec(v.shape, lambda i: (0, 0))

    return pl.pallas_call(
        finish,
        grid=(1,),
        in_specs=[whole(v) for v in (mixed, sums, late, weight)],
        out_specs=[whole(mixed), whole(late)],
        out_shape=[jax.ShapeDtypeStruct(v.shape, v.dtype) for v in (mixed, late)],
        name="hand_over",
    )(mixed, sums, late, weight)


def on_device(*operands):
    (
        u, logs, losses, eigen, frequency, group_in, group_out, feed, mixer_scale, mixer_weight,
        x, gain, routes, chosen, gate, up, down, shared_gate, shared_up, shared_down,
    ) = operands
    n_ep, n_tp = lax.axis_size("ep"), lax.axis_size("tp")
    positions, channels = u.shape
    groups, states = eigen.shape
    lanes_all = groups * states
    tiles = lanes_all // LANES
    token_rows, width = x.shape
    hidden, columns = gate.shape[2], down.shape[2]
    group_in = group_in.transpose(0, 1, 3, 2).reshape(2, channels, states)
    group_out = group_out.reshape(2, channels, states)
    feed = feed.reshape(1, channels)
    mixer_scale = mixer_scale.reshape((1, -1) if channels % LANES == 0 else (n_tp, channels))
    gain = gain.reshape(1, width)
    routes, chosen = routes.T, chosen.T
    given = (
        u, logs, losses, eigen, frequency, group_in, group_out, feed, mixer_scale, mixer_weight,
        x, gain, routes, chosen, gate, up, down, shared_gate, shared_up, shared_down,
    )
    local = [
        pltpu.VMEM(g.shape[1:] if k in (14, 15, 16) else g.shape, g.dtype) for k, g in enumerate(given)
    ]
    slot = -(-groups // 16) * 16
    wide = pltpu.VMEM((positions, lanes_all), f32)
    dma = pltpu.SemaphoreType.DMA
    scratch = local + [
        pltpu.VMEM((n_ep, token_rows, width), bf16),
        pltpu.VMEM((n_ep + 1, 2, n_tp // 2, token_rows, hidden), bf16),
        pltpu.VMEM((n_ep, token_rows, columns), bf16),
        pltpu.VMEM((n_ep, token_rows, columns), bf16),
        pltpu.VMEM((n_ep, 4, tiles, LANES), f32),
        pltpu.VMEM((2, n_tp // 2, positions, channels), bf16),
        pltpu.VMEM((positions, channels), bf16),
        pltpu.VMEM((2, 3 * slot, positions), bf16),
        pltpu.VMEM((tiles, LANES), f32),
        pltpu.VMEM((tiles, LANES), f32),
        pltpu.VMEM((2, channels, lanes_all), bf16),
        pltpu.VMEM((2, channels, lanes_all), bf16),
        wide, wide, wide, wide,
        pltpu.VMEM((4, ROWS, tiles, LANES), f32),
        pltpu.VMEM((4, ROWS, tiles, LANES), f32),
        pltpu.VMEM((2, tiles, LANES), f32),
        pltpu.VMEM((positions, channels), f32),
        pltpu.VMEM((token_rows, columns), f32),
        pltpu.VMEM((token_rows, n_ep), f32),
        dma((len(given),)),
        dma((n_ep // 2, PIECES)), dma((n_ep // 2, PIECES)), dma((1,)),
        dma((1,)), dma((n_ep, PIECES)), dma((n_ep, PIECES)),
        dma((1,)), dma((1,)), dma((n_ep + 1,)), dma((n_ep + 1,)),
        dma((1,)), dma((n_ep,)), dma((2,)),
        dma((4,)),
        dma((3,)),
        pltpu.VMEM((positions, columns), bf16),
        pltpu.VMEM((token_rows, LANES), f32),
    ]
    parts_out = pl.pallas_call(
        functools.partial(body, n_ep, n_tp),
        out_shape=[
            jax.ShapeDtypeStruct((positions, columns), bf16),
            jax.ShapeDtypeStruct((token_rows, columns), f32),
            jax.ShapeDtypeStruct((token_rows, columns), bf16),
            jax.ShapeDtypeStruct((token_rows, LANES), f32),
        ],
        in_specs=[pl.BlockSpec(memory_space=pl.ANY)] * len(given),
        out_specs=[pl.BlockSpec(memory_space=pl.ANY)] * 4,
        scratch_shapes=scratch,
        compiler_params=pltpu.CompilerParams(
            collective_id=0, has_side_effects=True, vmem_limit_bytes=VMEM_BYTES
        ),
        name="both_batches",
    )(*given)
    return hand_over(*parts_out)


def solution(mesh):
    return jax.shard_map(
        on_device,
        mesh=mesh,
        in_specs=(
            P("ep", "tp"),
            P("tp", "ep"),
            P("tp", "ep"),
            P("tp", None),
            P("tp", None),
            P(None, "tp", None, None),
            P(None, "tp", None, None),
            P("tp"),
            P(),
            P(None, "tp"),
            P("ep", None),
            P(),
            P("ep", None),
            P("ep", None),
            P("ep", None, "tp"),
            P("ep", None, "tp"),
            P("ep", None, "tp"),
            P(None, "tp"),
            P(None, "tp"),
            P(None, "tp"),
        ),
        out_specs=(P("ep", "tp"), P("ep", "tp")),
        check_vma=False,
    )
```
